256 devices in a mesh: grp: 2 (over y), sp: 16 (over z), tp: 8 (over x, core).
Axes of the slice: x: 4, y: 2, z: 16, core: 2. Of those that a mesh axis runs over, the one named last changes fastest.
The devices are a block of a 4x16x16 slice.
Arguments:
- tokens: bfloat16 [32768, 2048], P(('grp', 'sp')), parts along dimension 0, may hold values from -6 to 6
- doc_ids: int32 [32768], P(('grp', 'sp')), parts along dimension 0, may hold values from 0 to 3, never falling along the last dimension, each value on 1 to 8192 neighbouring positions
- gains: bfloat16 [2, 2048], replicated, may hold values from 0.099609375 to 1.8984375
- w_query: bfloat16 [2, 2048, 1024], P(None, None, 'tp'), may hold values from -0.125 to 0.125
- w_key: bfloat16 [2, 2048, 1024], P(None, None, 'tp'), may hold values from -0.125 to 0.125
- w_value: bfloat16 [2, 2048, 1024], P(None, None, 'tp'), may hold values from -0.125 to 0.125
- rel_table: float32 [2, 16, 257], P(None, 'tp'), may hold values from -6 to 270
- out_first: bfloat16 [1024, 2048], replicated, may hold values from -0.5 to 0.5
- out_last: bfloat16 [1024, 2048], P(None, 'tp'), may hold values from -0.5 to 0.5
Outputs:
- mixed: bfloat16 [32768, 2048], P(('grp', 'sp'), 'tp'), parts along dimension 0
The draws below stay inside these ranges and needn't reach their ends.
There are 2 independent parts, one for each index of `grp`. The reference program is written for one: setup_inputs(seed, part) draws one part's arguments, and reference() takes and returns one part's arrays. A program takes and returns all parts, laid end to end along the dimension named above; an argument that names none is the same for every part. Nothing has to cross between parts.
Inputs may be any that keep to these rules, and one draw needn't show every extreme that they name: `doc_ids`: document numbers never fall along the sequence.
All inputs are finite; a program needn't handle non-finite values.
Results may differ from the reference program's by a relative error of at most 0.014.
Values may be sent and summed in bfloat16 or wider, within the bound.
No kernel may reach another device: no remote copies, remote signals or barrier semaphores. Data moves between devices by JAX's collectives and lax.ppermute only.
A program may use at most 128 MiB of HBM per device.

```python
import math
import jax
import jax.numpy as jnp
import numpy as np
from jax import lax

D = 2048
HEADS = 16
HEAD_DIM = 64
SEG = 64
PREV_SEGS = 8
MAX_REL = 128
LAYERS = 2
TOKENS = 16384
DOCS = 4


def draw_rel_table(key, part):
    shape = (LAYERS, HEADS, 2 * MAX_REL + 1)
    return jnp.clip(jax.random.normal(key, shape, jnp.float32), -4.0, 4.0)


def shard_levels(stream_key, dims, shards, smallest, largest):
    def one(position, parts):
        heights = jax.random.uniform(jax.random.fold_in(jax.random.fold_in(stream_key, 6), position), (parts,), jnp.float32, smallest / len(shards), largest / len(shards))
        return jnp.repeat(jnp.exp(heights), dims[position] // parts).reshape((-1,) + (1,) * (len(dims) - position - 1))

    factor_of = one(*shards[0])
    for cut in shards[1:]:
        factor_of = factor_of * one(*cut)
    return factor_of


def profile(count, total, limit, skew):
    weights = [(1 << 20) // math.isqrt(rank ** skew) + 1 for rank in range(2, count + 1)]
    surplus, counts = total - limit - (count - 1), [1] * (count - 1)
    while surplus > 0:
        movable = [i for i in range(count - 1) if counts[i] < limit]
        whole, remaining = sum([weights[i] for i in movable]), surplus
        for i in movable:
            addition = min(limit - counts[i], max(1, remaining * weights[i] // whole), surplus)
            counts[i] = counts[i] + addition
            surplus = surplus - addition
    return np.array([limit] + counts)


def ragged_sizes(stream_key, count, total, limit, lean):
    if count == 2:
        one = jax.random.randint(stream_key, (), max(1, total - limit), min(limit, total - 1) + 1)
        return jnp.stack([one, total - one])
    tallies = jnp.asarray(profile(count, total, limit, lean), jnp.int32)
    pairs = (count - 1) // 2
    source_of, taker = tallies[1:1 + 2 * pairs:2], tallies[2:2 + 2 * pairs:2]
    room = jnp.minimum(source_of - 1, limit - taker)
    passed = jax.random.randint(jax.random.fold_in(stream_key, 1), (pairs,), 0, 1 << 20) % (room + 1)
    tallies = tallies.at[1:1 + 2 * pairs:2].set(source_of - passed).at[2:2 + 2 * pairs:2].set(taker + passed)
    return tallies[jax.random.permutation(jax.random.fold_in(stream_key, 2), count)]


def gaussian(rng, shape, scale, most, pieces=(), kind=jnp.bfloat16):
    array = scale * jax.random.normal(rng, shape, jnp.float32)
    if pieces:
        array = array * shard_levels(rng, shape, pieces, -0.22, 0.18)
    return jnp.clip(array, -most, most).astype(kind)


def setup_inputs(seed: int = 0, part: int = 0) -> dict:
    splits = jax.random.split(jax.random.key(seed), 10)
    part_splits = jax.random.split(jax.random.fold_in(splits[9], part), 10)
    tokens = gaussian(part_splits[0], (TOKENS, D), 1.0, 6.0, ((0, 16),))
    doc_ids = jnp.searchsorted(jnp.cumsum(ragged_sizes(part_splits[1], DOCS, TOKENS, TOKENS // 2, 1)), jnp.arange(TOKENS), side="right").astype(jnp.int32)
    gains = jnp.clip(1.0 + 0.18 * jax.random.normal(splits[2], (LAYERS, D), jnp.float32), 0.099609375, 1.8984375).astype(jnp.bfloat16)
    w_query = gaussian(splits[3], (LAYERS, D, HEADS * HEAD_DIM), D ** -0.5, 0.125, ((2, 8),))
    w_key = gaussian(splits[4], (LAYERS, D, HEADS * HEAD_DIM), D ** -0.5, 0.125, ((2, 8),))
    w_value = gaussian(splits[5], (LAYERS, D, HEADS * HEAD_DIM), D ** -0.5, 0.125, ((2, 8),))
    rel_table = draw_rel_table(jax.random.fold_in(splits[9], 71), part)
    out_first = gaussian(splits[7], (HEADS * HEAD_DIM, D), (HEADS * HEAD_DIM // 9) ** -0.5, 0.5)
    out_last = gaussian(splits[8], (HEADS * HEAD_DIM, D), (HEADS * HEAD_DIM // 9) ** -0.5, 0.5, ((1, 8),))
    return {"tokens": tokens, "doc_ids": doc_ids, "gains": gains, "w_query": w_query, "w_key": w_key, "w_value": w_value, "rel_table": rel_table, "out_first": out_first, "out_last": out_last}


def normalize(stream, gain_row):
    values32 = stream.astype(jnp.float32)
    scaled = values32 * lax.rsqrt(lax.optimization_barrier(jnp.mean(values32 * values32, axis=-1, keepdims=True)) + 1e-06)
    return (scaled * gain_row.astype(jnp.float32)).astype(jnp.bfloat16)

def banded(key_rows, seg_count):
    by_segment = key_rows.reshape((seg_count + PREV_SEGS, SEG) + key_rows.shape[1:])
    stacked = jnp.stack([by_segment[offset_seg:offset_seg + seg_count] for offset_seg in range(PREV_SEGS + 1)], axis=1)
    return stacked.reshape((seg_count, (PREV_SEGS + 1) * SEG) + key_rows.shape[1:])

def attend(queries, pad_keys, pad_values, query_docs, pad_docs, bias_table):
    seq_rows = queries.shape[0]
    seg_count = seq_rows // SEG
    head_count = bias_table.shape[0]
    head_width = queries.shape[1] // head_count
    band_rows = (PREV_SEGS + 1) * SEG
    query_blocks = queries.reshape(seg_count, SEG, head_count, head_width).astype(jnp.float32)
    key_band = banded(pad_keys.reshape(-1, head_count, head_width), seg_count).astype(jnp.float32)
    value_band = banded(pad_values.reshape(-1, head_count, head_width), seg_count).astype(jnp.float32)
    query_pos = jnp.arange(SEG, dtype=jnp.int32)[:, None]
    band_pos = jnp.arange(band_rows, dtype=jnp.int32)[None, :]
    rel_index = jnp.clip(PREV_SEGS * SEG + query_pos - band_pos, -MAX_REL, MAX_REL) + MAX_REL
    bias = jnp.take(bias_table.astype(jnp.float32), rel_index, axis=1)
    scores = jnp.einsum('nqhd,nkhd->nhqk', query_blocks, key_band) * head_width ** (-0.5) + bias[None]
    doc_band = banded(pad_docs, seg_count)
    allowed = doc_band[:, None, None, :] == query_docs.reshape(seg_count, 1, SEG, 1)
    scores = jnp.where(allowed, scores, jnp.float32(-1e+30))
    row_max = lax.optimization_barrier(jnp.max(scores, axis=-1, keepdims=True))
    exp_scores = jnp.exp(scores - row_max)
    probs = exp_scores / lax.optimization_barrier(jnp.sum(exp_scores, axis=-1, keepdims=True))
    weights = probs.astype(jnp.bfloat16).astype(jnp.float32)
    result = jnp.einsum('nhqk,nkhd->nqhd', weights, value_band)
    return result.astype(jnp.bfloat16).reshape(seq_rows, head_count * head_width)

def reference(tokens, doc_ids, gains, w_query, w_key, w_value, rel_table, out_first, out_last):
    reach_rows = PREV_SEGS * SEG
    pad_docs = jnp.concatenate([jnp.full((reach_rows,), -1, jnp.int32), doc_ids.astype(jnp.int32)])
    hidden = tokens
    for layer_number in range(LAYERS):
        normed = normalize(hidden, gains[layer_number])
        queries = jnp.dot(normed, w_query[layer_number], preferred_element_type=jnp.float32).astype(jnp.bfloat16)
        keys = jnp.dot(normed, w_key[layer_number], preferred_element_type=jnp.float32).astype(jnp.bfloat16)
        values = jnp.dot(normed, w_value[layer_number], preferred_element_type=jnp.float32).astype(jnp.bfloat16)
        blank = jnp.zeros((reach_rows, keys.shape[1]), jnp.bfloat16)
        attended = attend(queries, jnp.concatenate([blank, keys]), jnp.concatenate([blank, values]), doc_ids, pad_docs, rel_table[layer_number])
        weight = out_first if layer_number == 0 else out_last
        update = jnp.dot(attended, weight, preferred_element_type=jnp.float32)
        hidden = (hidden.astype(jnp.float32) + update).astype(jnp.bfloat16)
    return hidden
```

```python
import functools

import jax
import jax.numpy as jnp
from jax import lax
from jax.experimental import pallas as pl
from jax.experimental.pallas import tpu as pltpu
from jax.sharding import PartitionSpec as P

SEG = 64
PREV_SEGS = 8
MAX_REL = 128
LAYERS = 2
REACH = PREV_SEGS * SEG
QUERY_ROWS = 2 * SEG
BAND = REACH + QUERY_ROWS
NEG = -1e30
EPS = 1e-06
DOC_ROWS = 16

F32 = jnp.float32
BF16 = jnp.bfloat16


def cost(flops, bytes_accessed, transcendentals=0):
    return pl.CostEstimate(
        flops=flops, bytes_accessed=bytes_accessed, transcendentals=transcendentals
    )


def project_heads(rows, gain, wq, wk, wv, q_scale):
    rows32 = rows.astype(F32)
    inv = lax.rsqrt(jnp.mean(rows32 * rows32, axis=-1, keepdims=True) + EPS)
    scaled = rows * gain
    queries = jnp.dot(scaled, wq, preferred_element_type=F32) * (inv * q_scale)
    wkv = jnp.concatenate([wk, wv], axis=1)
    kv = jnp.dot(scaled, wkv, preferred_element_type=F32) * inv
    return queries.astype(BF16), kv.astype(BF16)


def store_kv(kv_ref, kv, docs_ref, step, block_rows):
    kv_ref[pl.ds(pl.multiple_of(step * block_rows, block_rows), block_rows), :] = kv
    if docs_ref is not None:

        @pl.when(step == 0)
        def _():
            width = kv_ref.shape[1]
            halves = [
                docs_ref[:, part * width : (part + 1) * width]
                for part in range(docs_ref.shape[1] // width)
            ]
            pad = jnp.zeros((DOC_ROWS - len(halves), width), F32)
            kv_ref[-DOC_ROWS:, :] = jnp.concatenate(halves + [pad], axis=0).astype(BF16)


def heads_kernel(q_scale, block_rows, *refs):
    x_ref, gain_ref, wq_ref, wk_ref, wv_ref, *rest = refs
    docs_ref = rest[0] if len(rest) == 3 else None
    q_ref, kv_ref = rest[-2:]
    queries, kv = project_heads(
        x_ref[...], gain_ref[...], wq_ref[...], wk_ref[...], wv_ref[...], q_scale
    )
    q_ref[...] = queries
    store_kv(kv_ref, kv, docs_ref, pl.program_id(0), block_rows)


def weight_specs(depth, width, layer):
    return [
        pl.BlockSpec((None, 1, depth), lambda i, *_: (layer, 0, 0)),
        *[pl.BlockSpec((None, depth, width), lambda i, *_: (layer, 0, 0)) for _ in range(3)],
    ]


def heads(tokens, gains, wq, wk, wv, docs, layer, half, half_rows, q_scale, block_rows=256):
    depth, width = wq.shape[1:]
    steps = half_rows // block_rows
    in_specs = [
        pl.BlockSpec((block_rows, depth), lambda i: (i + half * steps, 0)),
        *weight_specs(depth, width, layer),
    ]
    args = [tokens, gains, wq, wk, wv]
    extra = 0
    if half == 1:
        in_specs.append(pl.BlockSpec((1, half_rows), lambda i: (0, half)))
        args.append(docs)
        extra = DOC_ROWS
    return pl.pallas_call(
        functools.partial(heads_kernel, q_scale, block_rows),
        grid=(steps,),
        in_specs=in_specs,
        out_specs=[
            pl.BlockSpec((block_rows, width), lambda i: (i, 0)),
            pl.BlockSpec((half_rows + extra, 2 * width), lambda i: (0, 0)),
        ],
        out_shape=[
            jax.ShapeDtypeStruct((half_rows, width), BF16),
            jax.ShapeDtypeStruct((half_rows + extra, 2 * width), BF16),
        ],
        cost_estimate=cost(6 * half_rows * depth * width, 2 * depth * (half_rows + 3 * width)),
        name="heads",
    )(*args)


def bias_kernel(line_ref, out_ref):
    width = line_ref.shape[1]
    row = lax.broadcasted_iota(jnp.int32, (QUERY_ROWS, BAND), 0)
    col = lax.broadcasted_iota(jnp.int32, (QUERY_ROWS, BAND), 1)
    upper = row >= SEG
    seen = jnp.logical_and(
        jnp.logical_or(jnp.logical_not(upper), col >= SEG),
        jnp.logical_or(upper, col < BAND - SEG),
    )
    for item in range(line_ref.shape[0]):
        lines = jnp.broadcast_to(line_ref[item : item + 1, :], (QUERY_ROWS, width))
        rolled = pltpu.roll(lines, 0, 1, stride=1, stride_axis=0)
        out_ref[item] = jnp.where(seen, rolled[:, :BAND], NEG)


def bias_blocks(rel_table):
    layers, head_count, table_width = rel_table.shape
    flipped = jnp.flip(rel_table[:, :, 1:], axis=2)
    far = jnp.broadcast_to(rel_table[:, :, -1:], (layers, head_count, REACH - MAX_REL))
    tail = jnp.broadcast_to(rel_table[:, :, -1:], (layers, head_count, QUERY_ROWS))
    line = jnp.concatenate([far, flipped, tail], axis=2).reshape(layers * head_count, -1)
    return pl.pallas_call(
        bias_kernel,
        out_shape=jax.ShapeDtypeStruct((layers * head_count, QUERY_ROWS, BAND), F32),
        cost_estimate=cost(layers * head_count * QUERY_ROWS * BAND * 4, 0),
        name="bias",
    )(line)


def attention_kernel(head_width, from_far, *refs):
    if from_far:
        q_ref, lo_ref, hi_ref, docs_ref, bias_ref, out_ref = refs
        docs_rows = lo_ref[-DOC_ROWS:, :].astype(F32)
        width = docs_rows.shape[1]
        parts = q_ref.shape[0] // width
        docs_lo = jnp.concatenate([docs_rows[i : i + 1] for i in range(parts)], axis=1)
        docs_hi = docs_ref[...]
    else:
        q_ref, lo_ref, hi_ref, docs_ref, bias_ref, out_ref = refs
        docs_lo = docs_ref[:, : q_ref.shape[0]]
        docs_hi = docs_ref[:, q_ref.shape[0] :]
    half_rows, width = q_ref.shape
    head_count = width // head_width
    lane = lax.broadcasted_iota(jnp.int32, (QUERY_ROWS, width), 1) // head_width
    square = (QUERY_ROWS, QUERY_ROWS)
    diagonal = lax.broadcasted_iota(jnp.int32, square, 0) == lax.broadcasted_iota(
        jnp.int32, square, 1
    )
    ones = jnp.ones((BAND, width), BF16)
    bias = [bias_ref[head] for head in range(head_count)]
    for block in range(half_rows // QUERY_ROWS):
        start = block * QUERY_ROWS
        stop = start + QUERY_ROWS
        kv = jnp.concatenate([lo_ref[start:half_rows, :], hi_ref[:stop, :]], axis=0)
        docs_keys = jnp.concatenate([docs_lo[:, start:], docs_hi[:, :stop]], axis=1)
        docs_queries = jnp.sum(
            jnp.where(diagonal, docs_hi[:, start:stop], 0.0), axis=1, keepdims=True
        )
        same = docs_keys == docs_queries
        queries = q_ref[start:stop, :]
        zero = jnp.zeros_like(queries)
        stacked = jnp.concatenate(
            [jnp.where(lane == head, queries, zero) for head in range(head_count)], axis=0
        )
        scores = lax.dot_general(
            stacked, kv[:, :width], (((1,), (1,)), ((), ())), preferred_element_type=F32
        )
        weights = []
        for head in range(head_count):
            part = scores[head * QUERY_ROWS : (head + 1) * QUERY_ROWS] + bias[head]
            part = jnp.where(same, part, NEG)
            top = jnp.max(part, axis=1, keepdims=True)
            weights.append(jnp.exp(part - top).astype(BF16))
        weights = jnp.concatenate(weights, axis=0)
        summed = jnp.dot(
            weights,
            jnp.concatenate([kv[:, width:], ones], axis=1),
            preferred_element_type=F32,
        )
        result = summed[:, :width] / summed[:, width:]
        mine = result[:QUERY_ROWS]
        for head in range(1, head_count):
            mine = jnp.where(lane == head, result[head * QUERY_ROWS : (head + 1) * QUERY_ROWS], mine)
        out_ref[start:stop, :] = mine.astype(BF16)


def attention(queries, lo, hi, docs, biases, layer, head_width, from_far):
    half_rows, width = queries.shape
    head_count = width // head_width
    return pl.pallas_call(
        functools.partial(attention_kernel, head_width, from_far),
        grid=(1,),
        in_specs=[
            pl.BlockSpec(queries.shape, lambda i: (0, 0)),
            pl.BlockSpec(lo.shape, lambda i: (0, 0)),
            pl.BlockSpec(hi.shape, lambda i: (0, 0)),
            pl.BlockSpec((1, half_rows if from_far else 2 * half_rows), lambda i: (0, 0)),
            pl.BlockSpec((head_count, QUERY_ROWS, BAND), lambda i: (layer, 0, 0)),
        ],
        out_specs=pl.BlockSpec(queries.shape, lambda i: (0, 0)),
        out_shape=jax.ShapeDtypeStruct(queries.shape, BF16),
        cost_estimate=cost(
            8 * half_rows * BAND * width, 4 * head_count * QUERY_ROWS * BAND, half_rows * BAND * 2
        ),
        name="attend",
    )(queries, lo, hi, docs, biases)


def gather(block):
    chips = lax.axis_size("tp") // 2
    pairs = [(x, core) for x in range(chips) for core in range(2)]

    def moved(array, by, other=False):
        return lax.ppermute(
            array,
            "tp",
            [
                (2 * x + core, 2 * ((x + by) % chips) + (1 - core if other else core))
                for x, core in pairs
            ],
        )

    received = [moved(block, by) for by in range(1, chips)]
    partner = moved(block, 0, True)
    partners = moved(jnp.stack(received), 0, True)
    return [block, partner, *received, partners]


def slots_of(me, chips):
    x, core = me // 2, me % 2
    others = [(x + chips - by) % chips for by in range(1, chips)]
    return [
        2 * x + core,
        2 * x + 1 - core,
        *[2 * other + core for other in others],
        *[2 * other + 1 - core for other in others],
    ]


def place(me_ref, block_refs, slots_ref):
    chips = slots_ref.shape[0] // 2
    arrays = [ref[...] for ref in block_refs[:-1]]
    arrays += [block_refs[-1][i] for i in range(chips - 1)]
    for slot, array in zip(slots_of(me_ref[0], chips), arrays):
        slots_ref[slot] = array
    return jnp.concatenate([slots_ref[i] for i in range(2 * chips)], axis=1)


def gathered_specs(blocks, block_rows):
    width = blocks[0].shape[1]
    specs = [pl.BlockSpec((block_rows, width), lambda i, *_: (i, 0)) for _ in blocks[:-1]]
    count = blocks[-1].shape[0]
    specs.append(pl.BlockSpec((count, block_rows, width), lambda i, *_: (0, i, 0)))
    return specs


def next_kernel(q_scale, block_rows, gathered_count, *refs):
    me_ref, *refs = refs
    block_refs, refs = refs[:gathered_count], refs[gathered_count:]
    x_ref, w_ref, gain_ref, wq_ref, wk_ref, wv_ref, *rest = refs
    docs_ref = rest[0] if len(rest) == 6 else None
    q_ref, kv_ref, own_ref, slots_ref, cols_ref = rest[-5:]
    attended = place(me_ref, block_refs, slots_ref)
    update = jnp.dot(attended, w_ref[...], preferred_element_type=F32)
    hidden = (x_ref[...].astype(F32) + update).astype(BF16)
    col_width = own_ref.shape[1]
    for part in range(cols_ref.shape[0]):
        cols_ref[part] = hidden[:, part * col_width : (part + 1) * col_width]
    own_ref[...] = cols_ref[me_ref[0]]
    queries, kv = project_heads(
        hidden, gain_ref[...], wq_ref[...], wk_ref[...], wv_ref[...], q_scale
    )
    q_ref[...] = queries
    store_kv(kv_ref, kv, docs_ref, pl.program_id(0), block_rows)


def next_heads(
    me, blocks, tokens, w_out, gains, wq, wk, wv, docs, layer, half, q_scale, block_rows=256
):
    half_rows, block_width = blocks[0].shape
    depth, width = wq.shape[1:]
    inner = w_out.shape[0]
    members = inner // block_width
    col_width = depth // members
    steps = half_rows // block_rows
    in_specs = [
        *gathered_specs(blocks, block_rows),
        pl.BlockSpec((block_rows, depth), lambda i, *_: (i + half * steps, 0)),
        pl.BlockSpec(w_out.shape, lambda i, *_: (0, 0)),
        *weight_specs(depth, width, layer),
    ]
    args = [*blocks, tokens, w_out, gains, wq, wk, wv]
    extra = 0
    if half == 1:
        in_specs.append(pl.BlockSpec((1, half_rows), lambda i, *_: (0, half)))
        args.append(docs)
        extra = DOC_ROWS
    return pl.pallas_call(
        functools.partial(next_kernel, q_scale, block_rows, len(blocks)),
        grid_spec=pltpu.PrefetchScalarGridSpec(
            num_scalar_prefetch=1,
            grid=(steps,),
            in_specs=in_specs,
            out_specs=[
                pl.BlockSpec((block_rows, width), lambda i, *_: (i, 0)),
                pl.BlockSpec((half_rows + extra, 2 * width), lambda i, *_: (0, 0)),
                pl.BlockSpec((block_rows, col_width), lambda i, *_: (i, 0)),
            ],
            scratch_shapes=[
                pltpu.VMEM((members, block_rows, block_width), BF16),
                pltpu.VMEM((members, block_rows, col_width), BF16),
            ],
        ),
        out_shape=[
            jax.ShapeDtypeStruct((half_rows, width), BF16),
            jax.ShapeDtypeStruct((half_rows + extra, 2 * width), BF16),
            jax.ShapeDtypeStruct((half_rows, col_width), BF16),
        ],
        cost_estimate=cost(
            2 * half_rows * depth * (inner + 3 * width),
            2 * depth * (half_rows + 3 * width + inner),
        ),
        name="next_heads",
    )(me, *args)


def last_kernel(gathered_count, *refs):
    me_ref, *refs = refs
    block_refs, refs = refs[:gathered_count], refs[gathered_count:]
    own_ref, w_ref = refs[:2]
    out_ref, slots_ref = refs[-2:]
    attended = place(me_ref, block_refs, slots_ref)
    update = jnp.dot(attended, w_ref[...], preferred_element_type=F32)
    out_ref[...] = (own_ref[...].astype(F32) + update).astype(BF16)


def last_update(me, blocks, own, w_out, earlier, half, block_rows=256):
    half_rows, block_width = blocks[0].shape
    inner, col_width = w_out.shape
    steps = half_rows // block_rows
    in_specs = [
        *gathered_specs(blocks, block_rows),
        pl.BlockSpec((block_rows, col_width), lambda i, *_: (i, 0)),
        pl.BlockSpec(w_out.shape, lambda i, *_: (0, 0)),
    ]
    args = [me, *blocks, own, w_out]
    aliases = {}
    if earlier is not None:
        in_specs.append(pl.BlockSpec(memory_space=pl.ANY))
        aliases = {len(args): 0}
        args.append(earlier)
    return pl.pallas_call(
        functools.partial(last_kernel, len(blocks)),
        grid_spec=pltpu.PrefetchScalarGridSpec(
            num_scalar_prefetch=1,
            grid=(steps,),
            in_specs=in_specs,
            out_specs=pl.BlockSpec((block_rows, col_width), lambda i, *_: (i + half * steps, 0)),
            scratch_shapes=[pltpu.VMEM((inner // block_width, block_rows, block_width), BF16)],
        ),
        out_shape=jax.ShapeDtypeStruct((2 * half_rows, col_width), BF16),
        input_output_aliases=aliases,
        cost_estimate=cost(
            2 * half_rows * inner * col_width, 2 * inner * (half_rows + col_width)
        ),
        name="last",
    )(*args)


def shards(tokens, doc_ids, gains, w_query, w_key, w_value, rel_table, out_first, out_last):
    row_count = tokens.shape[0]
    half_rows = row_count // 2
    head_count = rel_table.shape[1]
    width = w_query.shape[2]
    head_width = width // head_count
    q_scale = head_width ** (-0.5)
    members = lax.axis_size("sp")
    onward = [(i, i + 1) for i in range(members - 1)]
    me = lax.axis_index("tp").astype(jnp.int32).reshape(1)
    docs = (doc_ids + 1).astype(F32).reshape(1, row_count)
    gains = gains[:, None, :]
    weights = (gains, w_query, w_key, w_value)

    q_late, kv_late = heads(tokens, *weights, docs, 0, 1, half_rows, q_scale)
    far = lax.ppermute(kv_late, "sp", onward)
    q_early, kv_early = heads(tokens, *weights, docs, 0, 0, half_rows, q_scale)
    biases = bias_blocks(rel_table)
    result = None
    for layer in range(LAYERS):
        late = attention(q_late, kv_early, kv_late, docs, biases, layer, head_width, False)
        late = gather(late)
        early = attention(q_early, far, kv_early, docs, biases, layer, head_width, True)
        early = gather(early)
        if layer == 0:
            q_late, kv_late, own_late = next_heads(
                me, late, tokens, out_first, *weights, docs, 1, 1, q_scale
            )
            far = lax.ppermute(kv_late, "sp", onward)
            q_early, kv_early, own_early = next_heads(
                me, early, tokens, out_first, *weights, docs, 1, 0, q_scale
            )
        else:
            result = last_update(me, late, own_late, out_last, None, 1)
            result = last_update(me, early, own_early, out_last, result, 0)
    return result


def solution(mesh):
    placed = (
        P(("grp", "sp"), None),
        P(("grp", "sp")),
        P(),
        P(None, None, "tp"),
        P(None, None, "tp"),
        P(None, None, "tp"),
        P(None, "tp", None),
        P(),
        P(None, "tp"),
    )
    return jax.shard_map(
        shards, mesh=mesh, in_specs=placed, out_specs=P(("grp", "sp"), "tp"), check_vma=False
    )
```

```python
import functools

import jax
import jax.numpy as jnp
from jax import lax
from jax.experimental import pallas as pl
from jax.experimental.pallas import tpu as pltpu
from jax.sharding import PartitionSpec as P

SEG = 64
PREV_SEGS = 8
MAX_REL = 128
LAYERS = 2
REACH = PREV_SEGS * SEG
QUERY_ROWS = 2 * SEG
BAND = REACH + QUERY_ROWS
NEG = -1e30
EPS = 1e-06
LOG2E = 1.4426950408889634
DOC_ROWS = 16
VMEM_LIMIT = 24 * 2**20
FIRST_VMEM_LIMIT = 51 * 2**20

F32 = jnp.float32
BF16 = jnp.bfloat16


def cost(flops, bytes_accessed, transcendentals=0):
    return pl.CostEstimate(
        flops=flops, bytes_accessed=bytes_accessed, transcendentals=transcendentals
    )


def project_heads(rows, gain, wq, wk, wv, q_scale):
    rows32 = rows.astype(F32)
    inv = lax.rsqrt(jnp.mean(rows32 * rows32, axis=-1, keepdims=True) + EPS)
    scaled = rows * gain
    queries = jnp.dot(scaled, wq, preferred_element_type=F32) * (inv * q_scale)
    wkv = jnp.concatenate([wk, wv], axis=1)
    kv = jnp.dot(scaled, wkv, preferred_element_type=F32) * inv
    return queries.astype(BF16), kv.astype(BF16)


def doc_rows(docs, width):
    parts = [docs[:, i : i + width] for i in range(0, docs.shape[1], width)]
    pad = jnp.zeros((DOC_ROWS - len(parts), width), F32)
    return jnp.concatenate(parts + [pad], axis=0).astype(BF16)


def heads_kernel(q_scale, block_rows, *refs):
    x_hbm, gain_hbm, *w_hbm, docs_hbm, table_hbm = refs[:7]
    q_ref, early_ref, late_ref, docs_ref, near_ref, gain_ref, *next_refs = refs[7:16]
    x_ref, *w_refs, ids_ref, table_ref, x_sem, w_sem, next_sem, side_sem = refs[16:]
    row_count = x_ref.shape[0]
    half_rows = row_count // 2
    order = [*range(half_rows, row_count, block_rows), *range(0, half_rows, block_rows)]
    side_copies = [
        pltpu.make_async_copy(source, target, side_sem.at[i])
        for i, (source, target) in enumerate(
            [(docs_hbm, ids_ref), (table_hbm, table_ref), (gain_hbm, gain_ref)]
        )
    ]
    w_copies = [
        pltpu.make_async_copy(w.at[0], w_ref, w_sem.at[i])
        for i, (w, w_ref) in enumerate(zip(w_hbm, w_refs))
    ]
    next_copies = [
        pltpu.make_async_copy(w.at[1], next_ref, next_sem.at[i])
        for i, (w, next_ref) in enumerate(zip(w_hbm, next_refs))
    ]
    x_copies = [
        pltpu.make_async_copy(
            x_hbm.at[pl.ds(row, block_rows)], x_ref.at[pl.ds(row, block_rows)], x_sem.at[i]
        )
        for i, row in enumerate(order)
    ]
    for copy in (*side_copies, x_copies[0], *w_copies, *x_copies[1:], *next_copies):
        copy.start()
    for copy in side_copies:
        copy.wait()
    near_bias(table_ref, near_ref)
    docs = (ids_ref[...] + 1).astype(F32)[None, :]
    docs_ref[...] = docs
    width = late_ref.shape[1]
    late_ref[half_rows:, :] = doc_rows(docs[:, half_rows:], width)
    for copy in w_copies:
        copy.wait()
    for copy, row in zip(x_copies, order):
        copy.wait()
        queries, kv = project_heads(
            x_ref[pl.ds(row, block_rows), :],
            gain_ref[0:1, :],
            *[w_ref[...] for w_ref in w_refs],
            q_scale,
        )
        q_ref[pl.ds(row, block_rows), :] = queries
        if row < half_rows:
            early_ref[pl.ds(row, block_rows), :] = kv
        else:
            late_ref[pl.ds(row - half_rows, block_rows), :] = kv
    for copy in next_copies:
        copy.wait()


def whole(count):
    return [pl.BlockSpec(memory_space=pltpu.VMEM)] * count


def heads(tokens, gains, wq, wk, wv, doc_ids, rel_table, q_scale, block_rows=256):
    row_count = tokens.shape[0]
    half_rows = row_count // 2
    depth, width = wq.shape[1:]
    items = rel_table.shape[0] * rel_table.shape[1]
    hbm = pl.BlockSpec(memory_space=pl.ANY)
    return pl.pallas_call(
        functools.partial(heads_kernel, q_scale, block_rows),
        in_specs=[hbm] * 7,
        out_specs=whole(9),
        out_shape=[
            jax.ShapeDtypeStruct((row_count, width), BF16),
            jax.ShapeDtypeStruct((half_rows, 2 * width), BF16),
            jax.ShapeDtypeStruct((half_rows + DOC_ROWS, 2 * width), BF16),
            jax.ShapeDtypeStruct((1, row_count), F32),
            jax.ShapeDtypeStruct((items, QUERY_ROWS, 2 * MAX_REL), F32),
            jax.ShapeDtypeStruct(gains.shape, BF16),
            *[jax.ShapeDtypeStruct((depth, width), BF16) for _ in range(3)],
        ],
        scratch_shapes=[
            pltpu.VMEM((row_count, depth), BF16),
            *[pltpu.VMEM((depth, width), BF16) for _ in range(3)],
            pltpu.VMEM(doc_ids.shape, doc_ids.dtype),
            pltpu.VMEM(rel_table.shape, F32),
            pltpu.SemaphoreType.DMA((row_count // block_rows,)),
            *[pltpu.SemaphoreType.DMA((3,)) for _ in range(3)],
        ],
        cost_estimate=cost(6 * row_count * depth * width, 2 * depth * (row_count + 3 * width)),
        compiler_params=pltpu.CompilerParams(vmem_limit_bytes=FIRST_VMEM_LIMIT),
        name="heads",
    )(tokens, gains, wq, wk, wv, doc_ids, rel_table)


def near_bias(table_ref, out_ref):
    layers, head_count, table_width = table_ref.shape
    near = 2 * MAX_REL
    width = near + QUERY_ROWS
    index = lax.broadcasted_iota(jnp.int32, (table_width, width), 0)
    place_of = lax.broadcasted_iota(jnp.int32, (table_width, width), 1)
    wanted = jnp.where(place_of < near, near - place_of, near)
    picked = (index == wanted).astype(F32)
    row = lax.broadcasted_iota(jnp.int32, (QUERY_ROWS, near), 0)
    col = lax.broadcasted_iota(jnp.int32, (QUERY_ROWS, near), 1)
    seen = jnp.logical_or(row >= SEG, col < near - SEG)
    for layer in range(layers):
        table = table_ref[layer]
        lines = jnp.dot(
            table, picked, precision=lax.Precision.HIGHEST, preferred_element_type=F32
        )
        lines = (lines - lines[:, near : near + 1]) * LOG2E
        for head in range(head_count):
            spread = jnp.broadcast_to(lines[head : head + 1, :], (QUERY_ROWS, width))
            rolled = pltpu.roll(spread, 0, 1, stride=1, stride_axis=0)
            out_ref[layer * head_count + head] = jnp.where(seen, rolled[:, :near], NEG)


def attention_kernel(head_width, layer, from_far, *refs):
    q_ref, lo_ref, hi_ref, docs_ref, bias_ref, out_ref = (*refs[:5], refs[-1])
    half_rows, width = out_ref.shape
    first_query = 0 if from_far else q_ref.shape[0] - half_rows
    if from_far:
        docs_rows = lo_ref[-DOC_ROWS:, :].astype(F32)
        parts = half_rows // docs_rows.shape[1]
        docs_lo = jnp.concatenate([docs_rows[i : i + 1] for i in range(parts)], axis=1)
        docs_hi = docs_ref[:, :half_rows]
    else:
        docs_lo = docs_ref[:, :half_rows]
        docs_hi = docs_ref[:, half_rows:]
    head_count = width // head_width
    lane = lax.broadcasted_iota(jnp.int32, (QUERY_ROWS, width), 1) // head_width
    square = (QUERY_ROWS, QUERY_ROWS)
    diagonal = lax.broadcasted_iota(jnp.int32, square, 0) == lax.broadcasted_iota(
        jnp.int32, square, 1
    )
    seen = jnp.logical_or(
        lax.broadcasted_iota(jnp.int32, square, 0) < SEG,
        lax.broadcasted_iota(jnp.int32, square, 1) >= SEG,
    )
    ones = jnp.ones((BAND, width), BF16)
    chunks = BAND // QUERY_ROWS
    plain = chunks - bias_ref.shape[2] // QUERY_ROWS
    first_head = layer * head_count
    for block in range(half_rows // QUERY_ROWS):
        start = block * QUERY_ROWS
        stop = start + QUERY_ROWS
        kv = jnp.concatenate([lo_ref[start:half_rows, :], hi_ref[:stop, :]], axis=0)
        docs_keys = jnp.concatenate([docs_lo[:, start:], docs_hi[:, :stop]], axis=1)
        docs_queries = jnp.sum(
            jnp.where(diagonal, docs_hi[:, start:stop], 0.0), axis=1, keepdims=True
        )
        same = []
        for c in range(chunks):
            keys = docs_keys[:, c * QUERY_ROWS : (c + 1) * QUERY_ROWS]
            if c == 0:
                keys = jnp.where(seen, keys, -1.0)
            same.append(keys == docs_queries)
        queries = q_ref[first_query + start : first_query + stop, :]
        zero = jnp.zeros_like(queries)
        stacked = jnp.concatenate(
            [jnp.where(lane == head, queries, zero) for head in range(head_count)], axis=0
        )
        scores = lax.dot_general(
            stacked, kv[:, :width], (((1,), (1,)), ((), ())), preferred_element_type=F32
        )
        weights = []
        for head in range(head_count):
            parts = []
            for c in range(chunks):
                part = scores[
                    head * QUERY_ROWS : (head + 1) * QUERY_ROWS,
                    c * QUERY_ROWS : (c + 1) * QUERY_ROWS,
                ]
                if c >= plain:
                    near = (c - plain) * QUERY_ROWS
                    part = part + bias_ref[first_head + head, :, near : near + QUERY_ROWS]
                parts.append(jnp.where(same[c], part, NEG))
            top = jnp.max(functools.reduce(jnp.maximum, parts), axis=1, keepdims=True)
            weights.append(
                jnp.concatenate([jnp.exp2(part - top).astype(BF16) for part in parts], axis=1)
            )
        weights = jnp.concatenate(weights, axis=0)
        summed = jnp.dot(
            weights,
            jnp.concatenate([kv[:, width:], ones], axis=1),
            preferred_element_type=F32,
        )
        result = summed[:, :width] / summed[:, width:]
        mine = result[:QUERY_ROWS]
        for head in range(1, head_count):
            mine = jnp.where(lane == head, result[head * QUERY_ROWS : (head + 1) * QUERY_ROWS], mine)
        out_ref[start:stop, :] = mine.astype(BF16)


def attention(queries, lo, hi, docs, biases, layer, head_width, from_far, ahead=()):
    half_rows = docs.shape[1] // 2
    width = queries.shape[1]
    return pl.pallas_call(
        functools.partial(attention_kernel, head_width, layer, from_far),
        in_specs=whole(5 + len(ahead)),
        out_specs=pl.BlockSpec(memory_space=pltpu.VMEM),
        out_shape=jax.ShapeDtypeStruct((half_rows, width), BF16),
        cost_estimate=cost(8 * half_rows * BAND * width, 8 * half_rows * width, half_rows * BAND * 2),
        compiler_params=pltpu.CompilerParams(vmem_limit_bytes=VMEM_LIMIT),
        name="attend",
    )(queries, lo, hi, docs, biases, *ahead)


def gather(block):
    chips = lax.axis_size("tp") // 2
    pairs = [(x, core) for x in range(chips) for core in range(2)]

    def moved(array, by, other=False):
        return lax.ppermute(
            array,
            "tp",
            [
                (2 * x + core, 2 * ((x + by) % chips) + (1 - core if other else core))
                for x, core in pairs
            ],
        )

    return moved, [block, *[moved(block, by) for by in range(1, chips)]]


def stack_kernel(*refs):
    out_ref = refs[-1]
    for i in range(out_ref.shape[0]):
        out_ref[i] = refs[i][...]


def from_partner(moved, blocks, after):
    stacked = pl.pallas_call(
        stack_kernel,
        in_specs=[*whole(len(blocks)), pl.BlockSpec(memory_space=pl.ANY)],
        out_specs=pl.BlockSpec(memory_space=pltpu.VMEM),
        out_shape=jax.ShapeDtypeStruct((len(blocks), *blocks[0].shape), BF16),
        compiler_params=pltpu.CompilerParams(vmem_limit_bytes=VMEM_LIMIT),
        name="stack",
    )(*blocks, after)
    return [*blocks, moved(stacked, 0, True)]


def slots_of(me, chips):
    x, core = me // 2, me % 2
    others = [(x + chips - by) % chips for by in range(1, chips)]
    return [
        2 * x + core,
        *[2 * other + core for other in others],
        2 * x + 1 - core,
        *[2 * other + 1 - core for other in others],
    ]


def place(me, block_refs, slots_ref):
    chips = slots_ref.shape[0] // 2
    arrays = [ref[...] for ref in block_refs[:-1]]
    arrays += [block_refs[-1][i] for i in range(chips)]
    for slot, array in zip(slots_of(me, chips), arrays):
        slots_ref[slot] = array


def rows_of(slots_ref, start, count):
    parts = [slots_ref[i, start : start + count, :] for i in range(slots_ref.shape[0])]
    return jnp.concatenate(parts, axis=1)


def next_kernel(q_scale, block_rows, gathered_count, half, *refs):
    me = lax.axis_index("tp")
    block_refs, refs = refs[:gathered_count], refs[gathered_count:]
    x_ref, w_ref, gain_ref, wq_ref, wk_ref, wv_ref, docs_ref, *rest = refs
    q_ref, kv_ref, own_ref, slots_ref, cols_ref = rest
    place(me, block_refs, slots_ref)
    half_rows, col_width = own_ref.shape
    first_row = half * half_rows
    if half == 1:
        kv_ref[half_rows:, :] = doc_rows(docs_ref[:, half_rows:], kv_ref.shape[1])
    for start in range(0, half_rows, block_rows):
        block = slice(start, start + block_rows)
        attended = rows_of(slots_ref, start, block_rows)
        update = jnp.dot(attended, w_ref[...], preferred_element_type=F32)
        rows = x_ref[first_row + start : first_row + start + block_rows, :]
        hidden = (rows.astype(F32) + update).astype(BF16)
        for part in range(cols_ref.shape[0]):
            cols_ref[part, block, :] = hidden[:, part * col_width : (part + 1) * col_width]
        queries, kv = project_heads(
            hidden, gain_ref[1:2, :], wq_ref[...], wk_ref[...], wv_ref[...], q_scale
        )
        q_ref[block, :] = queries
        kv_ref[block, :] = kv
    own_ref[...] = cols_ref[me]


def next_heads(blocks, tokens, w_out, gains, wq, wk, wv, docs, half, q_scale, block_rows=256):
    half_rows, block_width = blocks[0].shape
    depth, width = wq.shape
    inner = w_out.shape[0]
    members = inner // block_width
    col_width = depth // members
    args = [*blocks, tokens, w_out, gains, wq, wk, wv, docs]
    return pl.pallas_call(
        functools.partial(next_kernel, q_scale, block_rows, len(blocks), half),
        in_specs=whole(len(args)),
        out_specs=whole(3),
        out_shape=[
            jax.ShapeDtypeStruct((half_rows, width), BF16),
            jax.ShapeDtypeStruct((half_rows + half * DOC_ROWS, 2 * width), BF16),
            jax.ShapeDtypeStruct((half_rows, col_width), BF16),
        ],
        scratch_shapes=[
            pltpu.VMEM((members, half_rows, block_width), BF16),
            pltpu.VMEM((members, half_rows, col_width), BF16),
        ],
        cost_estimate=cost(
            2 * half_rows * depth * (inner + 3 * width),
            2 * depth * (half_rows + 3 * width + inner),
        ),
        compiler_params=pltpu.CompilerParams(vmem_limit_bytes=VMEM_LIMIT),
        name="next_heads",
    )(*args)


def last_kernel(gathered_count, *refs):
    block_refs, refs = refs[:gathered_count], refs[gathered_count:]
    own_ref, w_ref, out_ref, slots_ref = refs[0], refs[1], refs[-2], refs[-1]
    place(lax.axis_index("tp"), block_refs, slots_ref)
    half_rows = own_ref.shape[0]
    attended = rows_of(slots_ref, 0, half_rows)
    update = jnp.dot(attended, w_ref[...], preferred_element_type=F32)
    out_ref[:half_rows, :] = (own_ref[...].astype(F32) + update).astype(BF16)
    if len(refs) == 5:
        out_ref[half_rows:, :] = refs[2][...]


def last_update(blocks, own, w_out, below=()):
    half_rows, block_width = blocks[0].shape
    inner, col_width = w_out.shape
    args = [*blocks, own, w_out, *below]
    rows = half_rows + sum(array.shape[0] for array in below)
    return pl.pallas_call(
        functools.partial(last_kernel, len(blocks)),
        in_specs=whole(len(args)),
        out_specs=pl.BlockSpec(memory_space=pltpu.VMEM),
        scratch_shapes=[pltpu.VMEM((inner // block_width, half_rows, block_width), BF16)],
        out_shape=jax.ShapeDtypeStruct((rows, col_width), BF16),
        cost_estimate=cost(
            2 * half_rows * inner * col_width, 2 * inner * (half_rows + col_width)
        ),
        compiler_params=pltpu.CompilerParams(vmem_limit_bytes=VMEM_LIMIT),
        name="last",
    )(*args)


def shards(tokens, doc_ids, gains, w_query, w_key, w_value, rel_table, out_first, out_last):
    row_count = tokens.shape[0]
    half_rows = row_count // 2
    head_count = rel_table.shape[1]
    width = w_query.shape[2]
    head_width = width // head_count
    q_scale = head_width ** (-0.5) * LOG2E
    members = lax.axis_size("sp")
    onward = [(i, i + 1) for i in range(members - 1)]

    queries, kv_early, kv_late, docs, biases, *weights = heads(
        tokens, gains, w_query, w_key, w_value, doc_ids, rel_table, q_scale
    )
    q_late = q_early = queries
    far = lax.ppermute(kv_late, "sp", onward)
    result = None
    for layer in range(LAYERS):
        late = attention(q_late, kv_early, kv_late, docs, biases, layer, head_width, False)
        moved, late = gather(late)
        ahead = (tokens, out_first) if layer == 0 else (out_last,)
        early = attention(q_early, far, kv_early, docs, biases, layer, head_width, True, ahead)
        late = from_partner(moved, late, early)
        moved, early = gather(early)
        if layer == 0:
            q_late, kv_late, own_late = next_heads(
                late, tokens, out_first, *weights, docs, 1, q_scale
            )
            far = lax.ppermute(kv_late, "sp", onward)
            early = from_partner(moved, early, kv_late)
            q_early, kv_early, own_early = next_heads(
                early, tokens, out_first, *weights, docs, 0, q_scale
            )
        else:
            below = last_update(late, own_late, out_last)
            early = from_partner(moved, early, below)
            result = last_update(early, own_early, out_last, (below,))
    return result


def solution(mesh):
    placed = (
        P(("grp", "sp"), None),
        P(("grp", "sp")),
        P(),
        P(None, None, "tp"),
        P(None, None, "tp"),
        P(None, None, "tp"),
        P(None, "tp", None),
        P(),
        P(None, "tp"),
    )
    return jax.shard_map(
        shards, mesh=mesh, in_specs=placed, out_specs=P(("grp", "sp"), "tp"), check_vma=False
    )
```

```python
import functools

import jax
import jax.numpy as jnp
from jax import lax
from jax.experimental import pallas as pl
from jax.experimental.pallas import tpu as pltpu
from jax.sharding import PartitionSpec as P


SEG = 64
PREV_SEGS = 8
MAX_REL = 128
LAYERS = 2
REACH = PREV_SEGS * SEG
QUERY_ROWS = 2 * SEG
BAND = REACH + QUERY_ROWS
NEG = -1e30
EPS = 1e-06
LOG2E = 1.4426950408889634
DOC_ROWS = 16
VMEM_LIMIT = 24 * 2**20
FIRST_VMEM_LIMIT = 51 * 2**20


F32 = jnp.float32
BF16 = jnp.bfloat16


def cost(flops, bytes_accessed, transcendentals=0):
    return pl.CostEstimate(
        flops=flops, bytes_accessed=bytes_accessed, transcendentals=transcendentals
    )


def project_heads(rows, gain, wq, wk, wv, q_scale):
    rows32 = rows.astype(F32)
    inv = lax.rsqrt(jnp.mean(rows32 * rows32, axis=-1, keepdims=True) + EPS)
    scaled = rows * gain
    queries = jnp.dot(scaled, wq, preferred_element_type=F32) * (inv * q_scale)
    wkv = jnp.concatenate([wk, wv], axis=1)
    kv = jnp.dot(scaled, wkv, preferred_element_type=F32) * inv
    return queries.astype(BF16), kv.astype(BF16)


def doc_rows(docs, width):
    parts = [docs[:, i : i + width] for i in range(0, docs.shape[1], width)]
    pad = jnp.zeros((DOC_ROWS - len(parts), width), F32)
    return jnp.concatenate(parts + [pad], axis=0).astype(BF16)


def heads_kernel(q_scale, block_rows, *refs):
    x_hbm, gain_hbm, *w_hbm, docs_hbm, table_hbm = refs[:7]
    q_ref, early_ref, late_ref, docs_ref, near_ref, gain_ref, *next_refs = refs[7:16]
    x_ref, *w_refs, ids_ref, table_ref, x_sem, w_sem, next_sem, side_sem = refs[16:]
    row_count = x_ref.shape[0]
    half_rows = row_count // 2
    order = [*range(half_rows, row_count, block_rows), *range(0, half_rows, block_rows)]
    side_copies = [
        pltpu.make_async_copy(source, target, side_sem.at[i])
        for i, (source, target) in enumerate(
            [(docs_hbm, ids_ref), (table_hbm, table_ref), (gain_hbm, gain_ref)]
        )
    ]
    w_copies = [
        pltpu.make_async_copy(w.at[0], w_ref, w_sem.at[i])
        for i, (w, w_ref) in enumerate(zip(w_hbm, w_refs))
    ]
    next_copies = [
        pltpu.make_async_copy(w.at[1], next_ref, next_sem.at[i])
        for i, (w, next_ref) in enumerate(zip(w_hbm, next_refs))
    ]
    x_copies = [
        pltpu.make_async_copy(
            x_hbm.at[pl.ds(row, block_rows)], x_ref.at[pl.ds(row, block_rows)], x_sem.at[i]
        )
        for i, row in enumerate(order)
    ]
    for copy in (*side_copies, x_copies[0], *w_copies, x_copies[1]):
        copy.start()
    for copy in side_copies:
        copy.wait()
    near_bias(table_ref, near_ref)
    docs = (ids_ref[...] + 1).astype(F32)[None, :]
    docs_ref[...] = docs
    width = late_ref.shape[1]
    late_ref[half_rows:, :] = doc_rows(docs[:, half_rows:], width)
    for copy in w_copies:
        copy.wait()
    later = [[copy] for copy in x_copies[2:]] + [next_copies, []]
    for copy, row, starting in zip(x_copies, order, later):
        copy.wait()
        for other in starting:
            other.start()
        queries, kv = project_heads(
            x_ref[pl.ds(row, block_rows), :],
            gain_ref[0:1, :],
            *[w_ref[...] for w_ref in w_refs],
            q_scale,
        )
        q_ref[pl.ds(row, block_rows), :] = queries
        if row < half_rows:
            early_ref[pl.ds(row, block_rows), :] = kv
        else:
            late_ref[pl.ds(row - half_rows, block_rows), :] = kv
    for copy in next_copies:
        copy.wait()


def whole(count):
    return [pl.BlockSpec(memory_space=pltpu.VMEM)] * count


def heads(tokens, gains, wq, wk, wv, doc_ids, rel_table, q_scale, block_rows=256):
    row_count = tokens.shape[0]
    half_rows = row_count // 2
    depth, width = wq.shape[1:]
    items = rel_table.shape[0] * rel_table.shape[1]
    hbm = pl.BlockSpec(memory_space=pl.ANY)
    return pl.pallas_call(
        functools.partial(heads_kernel, q_scale, block_rows),
        in_specs=[hbm] * 7,
        out_specs=whole(9),
        out_shape=[
            jax.ShapeDtypeStruct((row_count, width), BF16),
            jax.ShapeDtypeStruct((half_rows, 2 * width), BF16),
            jax.ShapeDtypeStruct((half_rows + DOC_ROWS, 2 * width), BF16),
            jax.ShapeDtypeStruct((1, row_count), F32),
            jax.ShapeDtypeStruct((items, QUERY_ROWS, 2 * MAX_REL), F32),
            jax.ShapeDtypeStruct(gains.shape, BF16),
            *[jax.ShapeDtypeStruct((depth, width), BF16) for _ in range(3)],
        ],
        scratch_shapes=[
            pltpu.VMEM((row_count, depth), BF16),
            *[pltpu.VMEM((depth, width), BF16) for _ in range(3)],
            pltpu.VMEM(doc_ids.shape, doc_ids.dtype),
            pltpu.VMEM(rel_table.shape, F32),
            pltpu.SemaphoreType.DMA((row_count // block_rows,)),
            *[pltpu.SemaphoreType.DMA((3,)) for _ in range(3)],
        ],
        cost_estimate=cost(6 * row_count * depth * width, 2 * depth * (row_count + 3 * width)),
        compiler_params=pltpu.CompilerParams(vmem_limit_bytes=FIRST_VMEM_LIMIT),
        name="heads",
    )(tokens, gains, wq, wk, wv, doc_ids, rel_table)


def near_bias(table_ref, out_ref):
    layers, head_count, table_width = table_ref.shape
    near = 2 * MAX_REL
    width = near + QUERY_ROWS
    index = lax.broadcasted_iota(jnp.int32, (table_width, width), 0)
    place_of = lax.broadcasted_iota(jnp.int32, (table_width, width), 1)
    wanted = jnp.where(place_of < near, near - place_of, near)
    picked = (index == wanted).astype(F32)
    row = lax.broadcasted_iota(jnp.int32, (QUERY_ROWS, near), 0)
    col = lax.broadcasted_iota(jnp.int32, (QUERY_ROWS, near), 1)
    seen = jnp.logical_or(row >= SEG, col < near - SEG)
    for layer in range(layers):
        table = table_ref[layer]
        lines = jnp.dot(
            table, picked, precision=lax.Precision.HIGHEST, preferred_element_type=F32
        )
        lines = (lines - lines[:, near : near + 1]) * LOG2E
        for head in range(head_count):
            spread = jnp.broadcast_to(lines[head : head + 1, :], (QUERY_ROWS, width))
            rolled = pltpu.roll(spread, 0, 1, stride=1, stride_axis=0)
            out_ref[layer * head_count + head] = jnp.where(seen, rolled[:, :near], NEG)


def attention_kernel(head_width, layer, from_far, *refs):
    q_ref, lo_ref, hi_ref, docs_ref, bias_ref, out_ref = (*refs[:5], refs[-1])
    half_rows, width = out_ref.shape
    first_query = 0 if from_far else q_ref.shape[0] - half_rows
    if from_far:
        docs_rows = lo_ref[-DOC_ROWS:, :].astype(F32)
        parts = half_rows // docs_rows.shape[1]
        docs_lo = jnp.concatenate([docs_rows[i : i + 1] for i in range(parts)], axis=1)
        docs_hi = docs_ref[:, :half_rows]
    else:
        docs_lo = docs_ref[:, :half_rows]
        docs_hi = docs_ref[:, half_rows:]
    head_count = width // head_width
    lane = lax.broadcasted_iota(jnp.int32, (QUERY_ROWS, width), 1) // head_width
    square = (QUERY_ROWS, QUERY_ROWS)
    diagonal = lax.broadcasted_iota(jnp.int32, square, 0) == lax.broadcasted_iota(
        jnp.int32, square, 1
    )
    seen = jnp.logical_or(
        lax.broadcasted_iota(jnp.int32, square, 0) < SEG,
        lax.broadcasted_iota(jnp.int32, square, 1) >= SEG,
    )
    ones = jnp.ones((BAND, width), BF16)
    chunks = BAND // QUERY_ROWS
    plain = chunks - bias_ref.shape[2] // QUERY_ROWS
    first_head = layer * head_count
    for block in range(half_rows // QUERY_ROWS):
        start = block * QUERY_ROWS
        stop = start + QUERY_ROWS
        kv = jnp.concatenate([lo_ref[start:half_rows, :], hi_ref[:stop, :]], axis=0)
        docs_keys = jnp.concatenate([docs_lo[:, start:], docs_hi[:, :stop]], axis=1)
        docs_queries = jnp.sum(
            jnp.where(diagonal, docs_hi[:, start:stop], 0.0), axis=1, keepdims=True
        )
        same = []
        for c in range(chunks):
            keys = docs_keys[:, c * QUERY_ROWS : (c + 1) * QUERY_ROWS]
            if c == 0:
                keys = jnp.where(seen, keys, -1.0)
            same.append(keys == docs_queries)
        queries = q_ref[first_query + start : first_query + stop, :]
        zero = jnp.zeros_like(queries)
        stacked = jnp.concatenate(
            [jnp.where(lane == head, queries, zero) for head in range(head_count)], axis=0
        )
        scores = lax.dot_general(
            stacked, kv[:, :width], (((1,), (1,)), ((), ())), preferred_element_type=F32
        )
        weights = []
        for head in range(head_count):
            parts = []
            for c in range(chunks):
                part = scores[
                    head * QUERY_ROWS : (head + 1) * QUERY_ROWS,
                    c * QUERY_ROWS : (c + 1) * QUERY_ROWS,
                ]
                if c >= plain:
                    near = (c - plain) * QUERY_ROWS
                    part = part + bias_ref[first_head + head, :, near : near + QUERY_ROWS]
                parts.append(jnp.where(same[c], part, NEG))
            top = jnp.max(functools.reduce(jnp.maximum, parts), axis=1, keepdims=True)
            weights.append(
                jnp.concatenate([jnp.exp2(part - top).astype(BF16) for part in parts], axis=1)
            )
        weights = jnp.concatenate(weights, axis=0)
        summed = jnp.dot(
            weights,
            jnp.concatenate([kv[:, width:], ones], axis=1),
            preferred_element_type=F32,
        )
        result = summed[:, :width] / summed[:, width:]
        mine = result[:QUERY_ROWS]
        for head in range(1, head_count):
            mine = jnp.where(lane == head, result[head * QUERY_ROWS : (head + 1) * QUERY_ROWS], mine)
        out_ref[start:stop, :] = mine.astype(BF16)


def attention(queries, lo, hi, docs, biases, layer, head_width, from_far, ahead=()):
    half_rows = docs.shape[1] // 2
    width = queries.shape[1]
    return pl.pallas_call(
        functools.partial(attention_kernel, head_width, layer, from_far),
        in_specs=whole(5 + len(ahead)),
        out_specs=pl.BlockSpec(memory_space=pltpu.VMEM),
        out_shape=jax.ShapeDtypeStruct((half_rows, width), BF16),
        cost_estimate=cost(8 * half_rows * BAND * width, 8 * half_rows * width, half_rows * BAND * 2),
        compiler_params=pltpu.CompilerParams(vmem_limit_bytes=VMEM_LIMIT),
        name="attend",
    )(queries, lo, hi, docs, biases, *ahead)


def gather(block):
    chips = lax.axis_size("tp") // 2
    pairs = [(x, core) for x in range(chips) for core in range(2)]

    def moved(array, by, other=False):
        return lax.ppermute(
            array,
            "tp",
            [
                (2 * x + core, 2 * ((x + by) % chips) + (1 - core if other else core))
                for x, core in pairs
            ],
        )

    blocks = [block]
    for by in range(1, chips):
        blocks.append(moved(block, by))
    return moved, blocks


def stack_kernel(*refs):
    out_ref = refs[-1]
    for i in range(out_ref.shape[0]):
        out_ref[i] = refs[i][...]


def from_partner(moved, blocks, after):
    stack = pl.pallas_call(
        stack_kernel,
        in_specs=[*whole(len(blocks)), pl.BlockSpec(memory_space=pl.ANY)],
        out_specs=pl.BlockSpec(memory_space=pltpu.VMEM),
        out_shape=jax.ShapeDtypeStruct((len(blocks), *blocks[0].shape), BF16),
        compiler_params=pltpu.CompilerParams(vmem_limit_bytes=VMEM_LIMIT),
        name="stack",
    )
    stacked = stack(*blocks, after)
    return [*blocks, moved(stacked, 0, True)]


def slots_of(me, chips):
    x, core = me // 2, me % 2
    others = [(x + chips - by) % chips for by in range(1, chips)]
    return [
        2 * x + core,
        *[2 * other + core for other in others],
        2 * x + 1 - core,
        *[2 * other + 1 - core for other in others],
    ]


def place(me, block_refs, slots_ref):
    chips = slots_ref.shape[0] // 2
    arrays = [ref[...] for ref in block_refs[:-1]]
    arrays += [block_refs[-1][i] for i in range(chips)]
    for slot, array in zip(slots_of(me, chips), arrays):
        slots_ref[slot] = array


def rows_of(slots_ref, start, count):
    parts = [slots_ref[i, start : start + count, :] for i in range(slots_ref.shape[0])]
    return jnp.concatenate(parts, axis=1)


def next_kernel(q_scale, block_rows, gathered_count, half, *refs):
    me = lax.axis_index("tp")
    block_refs, refs = refs[:gathered_count], refs[gathered_count:]
    x_ref, w_ref, gain_ref, wq_ref, wk_ref, wv_ref, docs_ref, *rest = refs
    q_ref, kv_ref, own_ref, slots_ref, cols_ref = rest
    place(me, block_refs, slots_ref)
    half_rows, col_width = own_ref.shape
    first_row = half * half_rows
    if half == 1:
        kv_ref[half_rows:, :] = doc_rows(docs_ref[:, half_rows:], kv_ref.shape[1])
    for start in range(0, half_rows, block_rows):
        block = slice(start, start + block_rows)
        attended = rows_of(slots_ref, start, block_rows)
        update = jnp.dot(attended, w_ref[...], preferred_element_type=F32)
        rows = x_ref[first_row + start : first_row + start + block_rows, :]
        hidden = (rows.astype(F32) + update).astype(BF16)
        for part in range(cols_ref.shape[0]):
            cols_ref[part, block, :] = hidden[:, part * col_width : (part + 1) * col_width]
        queries, kv = project_heads(
            hidden, gain_ref[1:2, :], wq_ref[...], wk_ref[...], wv_ref[...], q_scale
        )
        q_ref[block, :] = queries
        kv_ref[block, :] = kv
    own_ref[...] = cols_ref[me]


def next_heads(blocks, tokens, w_out, gains, wq, wk, wv, docs, half, q_scale, block_rows=256):
    half_rows, block_width = blocks[0].shape
    depth, width = wq.shape
    inner = w_out.shape[0]
    members = inner // block_width
    col_width = depth // members
    args = [*blocks, tokens, w_out, gains, wq, wk, wv, docs]
    return pl.pallas_call(
        functools.partial(next_kernel, q_scale, block_rows, len(blocks), half),
        in_specs=whole(len(args)),
        out_specs=whole(3),
        out_shape=[
            jax.ShapeDtypeStruct((half_rows, width), BF16),
            jax.ShapeDtypeStruct((half_rows + half * DOC_ROWS, 2 * width), BF16),
            jax.ShapeDtypeStruct((half_rows, col_width), BF16),
        ],
        scratch_shapes=[
            pltpu.VMEM((members, half_rows, block_width), BF16),
            pltpu.VMEM((members, half_rows, col_width), BF16),
        ],
        cost_estimate=cost(
            2 * half_rows * depth * (inner + 3 * width),
            2 * depth * (half_rows + 3 * width + inner),
        ),
        compiler_params=pltpu.CompilerParams(vmem_limit_bytes=VMEM_LIMIT),
        name="next_heads",
    )(*args)


def last_kernel(gathered_count, *refs):
    block_refs, refs = refs[:gathered_count], refs[gathered_count:]
    own_ref, w_ref, out_ref, slots_ref = refs[0], refs[1], refs[-2], refs[-1]
    place(lax.axis_index("tp"), block_refs, slots_ref)
    half_rows = own_ref.shape[0]
    attended = rows_of(slots_ref, 0, half_rows)
    update = jnp.dot(attended, w_ref[...], preferred_element_type=F32)
    out_ref[:half_rows, :] = (own_ref[...].astype(F32) + update).astype(BF16)
    if len(refs) == 5:
        out_ref[half_rows:, :] = refs[2][...]


def last_update(blocks, own, w_out, below=()):
    half_rows, block_width = blocks[0].shape
    inner, col_width = w_out.shape
    args = [*blocks, own, w_out, *below]
    rows = half_rows + sum(array.shape[0] for array in below)
    return pl.pallas_call(
        functools.partial(last_kernel, len(blocks)),
        in_specs=whole(len(args)),
        out_specs=pl.BlockSpec(memory_space=pltpu.VMEM),
        scratch_shapes=[pltpu.VMEM((inner // block_width, half_rows, block_width), BF16)],
        out_shape=jax.ShapeDtypeStruct((rows, col_width), BF16),
        cost_estimate=cost(
            2 * half_rows * inner * col_width, 2 * inner * (half_rows + col_width)
        ),
        compiler_params=pltpu.CompilerParams(vmem_limit_bytes=VMEM_LIMIT),
        name="last",
    )(*args)


def shards(tokens, doc_ids, gains, w_query, w_key, w_value, rel_table, out_first, out_last):
    head_count = rel_table.shape[1]
    width = w_query.shape[2]
    head_width = width // head_count
    q_scale = head_width ** (-0.5) * LOG2E
    members = lax.axis_size("sp")
    onward = [(i, i + 1) for i in range(members - 1)]

    queries, kv_early, kv_late, docs, biases, *weights = heads(
        tokens, gains, w_query, w_key, w_value, doc_ids, rel_table, q_scale
    )
    q_late = q_early = queries
    far = lax.ppermute(kv_late, "sp", onward)
    result = None
    for layer in range(LAYERS):
        late = attention(q_late, kv_early, kv_late, docs, biases, layer, head_width, False)
        moved, late = gather(late)
        ahead = (tokens, out_first) if layer == 0 else (out_last,)
        early = attention(
            q_early, far, kv_early, docs, biases, layer, head_width, True, ahead
        )
        late = from_partner(moved, late, early)
        moved, early = gather(early)
        if layer == 0:
            q_late, kv_late, own_late = next_heads(
                late, tokens, out_first, *weights, docs, 1, q_scale
            )
            far = lax.ppermute(kv_late, "sp", onward)
            early = from_partner(moved, early, kv_late)
            q_early, kv_early, own_early = next_heads(
                early, tokens, out_first, *weights, docs, 0, q_scale
            )
        else:
            below = last_update(late, own_late, out_last)
            early = from_partner(moved, early, below)
            result = last_update(early, own_early, out_last, (below,))
    return result


def solution(mesh):
    placed = (
        P(("grp", "sp"), None),
        P(("grp", "sp")),
        P(),
        P(None, None, "tp"),
        P(None, None, "tp"),
        P(None, None, "tp"),
        P(None, "tp", None),
        P(),
        P(None, "tp"),
    )
    return jax.shard_map(
        shards, mesh=mesh, in_specs=placed, out_specs=P(("grp", "sp"), "tp"), check_vma=False
    )
```

```python
import functools

import jax
import jax.numpy as jnp
from jax import lax
from jax.experimental import pallas as pl
from jax.experimental.pallas import tpu as pltpu
from jax.sharding import PartitionSpec as P


SEG = 64
PREV_SEGS = 8
MAX_REL = 128
LAYERS = 2
REACH = PREV_SEGS * SEG
QUERY_ROWS = 2 * SEG
BAND = REACH + QUERY_ROWS
NEG = -1e30
EPS = 1e-06
LOG2E = 1.4426950408889634
DOC_ROWS = 16
VMEM_LIMIT = 24 * 2**20
FIRST_VMEM_LIMIT = 51 * 2**20


F32 = jnp.float32
BF16 = jnp.bfloat16


def cost(flops, bytes_accessed, transcendentals=0):
    return pl.CostEstimate(
        flops=flops, bytes_accessed=bytes_accessed, transcendentals=transcendentals
    )


def project_heads(rows, gain, wq, wk, wv, q_scale):
    rows32 = rows.astype(F32)
    inv = lax.rsqrt(jnp.mean(rows32 * rows32, axis=-1, keepdims=True) + EPS)
    scaled = rows * gain
    queries = jnp.dot(scaled, wq, preferred_element_type=F32) * (inv * q_scale)
    wkv = jnp.concatenate([wk, wv], axis=1)
    kv = jnp.dot(scaled, wkv, preferred_element_type=F32) * inv
    return queries.astype(BF16), kv.astype(BF16)


def doc_rows(docs, width):
    parts = [docs[:, i : i + width] for i in range(0, docs.shape[1], width)]
    pad = jnp.zeros((DOC_ROWS - len(parts), width), F32)
    return jnp.concatenate(parts + [pad], axis=0).astype(BF16)


def heads_kernel(q_scale, block_rows, *refs):
    x_hbm, gain_hbm, *w_hbm, docs_hbm, table_hbm = refs[:7]
    q_ref, early_ref, late_ref, docs_ref, near_ref, gain_ref, *next_refs = refs[7:16]
    x_ref, *w_refs, ids_ref, table_ref, x_sem, w_sem, next_sem, side_sem = refs[16:]
    row_count = x_ref.shape[0]
    half_rows = row_count // 2
    order = [*range(half_rows, row_count, block_rows), *range(0, half_rows, block_rows)]
    side_copies = [
        pltpu.make_async_copy(source, target, side_sem.at[i])
        for i, (source, target) in enumerate(
            [(docs_hbm, ids_ref), (table_hbm, table_ref), (gain_hbm, gain_ref)]
        )
    ]
    w_copies = [
        pltpu.make_async_copy(w.at[0], w_ref, w_sem.at[i])
        for i, (w, w_ref) in enumerate(zip(w_hbm, w_refs))
    ]
    next_copies = [
        pltpu.make_async_copy(w.at[1], next_ref, next_sem.at[i])
        for i, (w, next_ref) in enumerate(zip(w_hbm, next_refs))
    ]
    x_copies = [
        pltpu.make_async_copy(
            x_hbm.at[pl.ds(row, block_rows)], x_ref.at[pl.ds(row, block_rows)], x_sem.at[i]
        )
        for i, row in enumerate(order)
    ]
    for copy in (*side_copies, x_copies[0], *w_copies, x_copies[1]):
        copy.start()
    for copy in side_copies:
        copy.wait()
    near_bias(table_ref, near_ref)
    docs = (ids_ref[...] + 1).astype(F32)[None, :]
    docs_ref[...] = docs
    width = late_ref.shape[1]
    late_ref[half_rows:, :] = doc_rows(docs[:, half_rows:], width)
    for copy in w_copies:
        copy.wait()
    later = [[copy] for copy in x_copies[2:]] + [next_copies, []]
    for copy, row, starting in zip(x_copies, order, later):
        copy.wait()
        for other in starting:
            other.start()
        queries, kv = project_heads(
            x_ref[pl.ds(row, block_rows), :],
            gain_ref[0:1, :],
            *[w_ref[...] for w_ref in w_refs],
            q_scale,
        )
        q_ref[pl.ds(row, block_rows), :] = queries
        if row < half_rows:
            early_ref[pl.ds(row, block_rows), :] = kv
        else:
            late_ref[pl.ds(row - half_rows, block_rows), :] = kv
    for copy in next_copies:
        copy.wait()


def whole(count):
    return [pl.BlockSpec(memory_space=pltpu.VMEM)] * count


def heads(tokens, gains, wq, wk, wv, doc_ids, rel_table, q_scale, block_rows=256):
    row_count = tokens.shape[0]
    half_rows = row_count // 2
    depth, width = wq.shape[1:]
    items = rel_table.shape[0] * rel_table.shape[1]
    hbm = pl.BlockSpec(memory_space=pltpu.HBM)
    args = [tokens, gains, wq, wk, wv, doc_ids, rel_table]
    args = [pltpu.with_memory_space_constraint(array, pltpu.HBM) for array in args]
    return pl.pallas_call(
        functools.partial(heads_kernel, q_scale, block_rows),
        in_specs=[hbm] * 7,
        out_specs=whole(9),
        out_shape=[
            jax.ShapeDtypeStruct((row_count, width), BF16),
            jax.ShapeDtypeStruct((half_rows, 2 * width), BF16),
            jax.ShapeDtypeStruct((half_rows + DOC_ROWS, 2 * width), BF16),
            jax.ShapeDtypeStruct((1, row_count), F32),
            jax.ShapeDtypeStruct((items, QUERY_ROWS, 2 * MAX_REL), F32),
            jax.ShapeDtypeStruct(gains.shape, BF16),
            *[jax.ShapeDtypeStruct((depth, width), BF16) for _ in range(3)],
        ],
        scratch_shapes=[
            pltpu.VMEM((row_count, depth), BF16),
            *[pltpu.VMEM((depth, width), BF16) for _ in range(3)],
            pltpu.VMEM(doc_ids.shape, doc_ids.dtype),
            pltpu.VMEM(rel_table.shape, F32),
            pltpu.SemaphoreType.DMA((row_count // block_rows,)),
            *[pltpu.SemaphoreType.DMA((3,)) for _ in range(3)],
        ],
        cost_estimate=cost(6 * row_count * depth * width, 2 * depth * (row_count + 3 * width)),
        compiler_params=pltpu.CompilerParams(vmem_limit_bytes=FIRST_VMEM_LIMIT),
        name="heads",
    )(*args)


def near_bias(table_ref, out_ref):
    layers, head_count, table_width = table_ref.shape
    near = 2 * MAX_REL
    width = near + QUERY_ROWS
    index = lax.broadcasted_iota(jnp.int32, (table_width, width), 0)
    place_of = lax.broadcasted_iota(jnp.int32, (table_width, width), 1)
    wanted = jnp.where(place_of < near, near - place_of, near)
    picked = (index == wanted).astype(F32)
    row = lax.broadcasted_iota(jnp.int32, (QUERY_ROWS, near), 0)
    col = lax.broadcasted_iota(jnp.int32, (QUERY_ROWS, near), 1)
    seen = jnp.logical_or(row >= SEG, col < near - SEG)
    for layer in range(layers):
        table = table_ref[layer]
        lines = jnp.dot(
            table, picked, precision=lax.Precision.HIGHEST, preferred_element_type=F32
        )
        lines = (lines - lines[:, near : near + 1]) * LOG2E
        for head in range(head_count):
            spread = jnp.broadcast_to(lines[head : head + 1, :], (QUERY_ROWS, width))
            rolled = pltpu.roll(spread, 0, 1, stride=1, stride_axis=0)
            out_ref[layer * head_count + head] = jnp.where(seen, rolled[:, :near], NEG)


def attention_kernel(head_width, layer, from_far, *refs):
    q_ref, lo_ref, hi_ref, docs_ref, bias_ref, out_ref = (*refs[:5], refs[-1])
    half_rows, width = out_ref.shape
    first_query = 0 if from_far else q_ref.shape[0] - half_rows
    if from_far:
        docs_rows = lo_ref[-DOC_ROWS:, :].astype(F32)
        parts = half_rows // docs_rows.shape[1]
        docs_lo = jnp.concatenate([docs_rows[i : i + 1] for i in range(parts)], axis=1)
        docs_hi = docs_ref[:, :half_rows]
    else:
        docs_lo = docs_ref[:, :half_rows]
        docs_hi = docs_ref[:, half_rows:]
    head_count = width // head_width
    lane = lax.broadcasted_iota(jnp.int32, (QUERY_ROWS, width), 1) // head_width
    square = (QUERY_ROWS, QUERY_ROWS)
    diagonal = lax.broadcasted_iota(jnp.int32, square, 0) == lax.broadcasted_iota(
        jnp.int32, square, 1
    )
    seen = jnp.logical_or(
        lax.broadcasted_iota(jnp.int32, square, 0) < SEG,
        lax.broadcasted_iota(jnp.int32, square, 1) >= SEG,
    )
    ones = jnp.ones((BAND, width), BF16)
    chunks = BAND // QUERY_ROWS
    plain = chunks - bias_ref.shape[2] // QUERY_ROWS
    first_head = layer * head_count
    for block in range(half_rows // QUERY_ROWS):
        start = block * QUERY_ROWS
        stop = start + QUERY_ROWS
        kv = jnp.concatenate([lo_ref[start:half_rows, :], hi_ref[:stop, :]], axis=0)
        docs_keys = jnp.concatenate([docs_lo[:, start:], docs_hi[:, :stop]], axis=1)
        docs_queries = jnp.sum(
            jnp.where(diagonal, docs_hi[:, start:stop], 0.0), axis=1, keepdims=True
        )
        same = []
        for c in range(chunks):
            keys = docs_keys[:, c * QUERY_ROWS : (c + 1) * QUERY_ROWS]
            if c == 0:
                keys = jnp.where(seen, keys, -1.0)
            same.append(keys == docs_queries)
        queries = q_ref[first_query + start : first_query + stop, :]
        zero = jnp.zeros_like(queries)
        stacked = jnp.concatenate(
            [jnp.where(lane == head, queries, zero) for head in range(head_count)], axis=0
        )
        scores = lax.dot_general(
            stacked, kv[:, :width], (((1,), (1,)), ((), ())), preferred_element_type=F32
        )
        weights = []
        for head in range(head_count):
            parts = []
            for c in range(chunks):
                part = scores[
                    head * QUERY_ROWS : (head + 1) * QUERY_ROWS,
                    c * QUERY_ROWS : (c + 1) * QUERY_ROWS,
                ]
                if c >= plain:
                    near = (c - plain) * QUERY_ROWS
                    part = part + bias_ref[first_head + head, :, near : near + QUERY_ROWS]
                parts.append(jnp.where(same[c], part, NEG))
            top = jnp.max(functools.reduce(jnp.maximum, parts), axis=1, keepdims=True)
            weights.append(
                jnp.concatenate([jnp.exp2(part - top).astype(BF16) for part in parts], axis=1)
            )
        weights = jnp.concatenate(weights, axis=0)
        summed = jnp.dot(
            weights,
            jnp.concatenate([kv[:, width:], ones], axis=1),
            preferred_element_type=F32,
        )
        result = summed[:, :width] / summed[:, width:]
        mine = result[:QUERY_ROWS]
        for head in range(1, head_count):
            mine = jnp.where(lane == head, result[head * QUERY_ROWS : (head + 1) * QUERY_ROWS], mine)
        out_ref[start:stop, :] = mine.astype(BF16)


def attention(queries, lo, hi, docs, biases, layer, head_width, from_far, ahead=()):
    half_rows = docs.shape[1] // 2
    width = queries.shape[1]
    return pl.pallas_call(
        functools.partial(attention_kernel, head_width, layer, from_far),
        in_specs=whole(5 + len(ahead)),
        out_specs=pl.BlockSpec(memory_space=pltpu.VMEM),
        out_shape=jax.ShapeDtypeStruct((half_rows, width), BF16),
        cost_estimate=cost(400 * half_rows * BAND * width, 8 * half_rows * width, half_rows * BAND * 2),
        compiler_params=pltpu.CompilerParams(vmem_limit_bytes=VMEM_LIMIT),
        name="attend",
    )(queries, lo, hi, docs, biases, *ahead)


def gather(block):
    chips = lax.axis_size("tp") // 2
    pairs = [(x, core) for x in range(chips) for core in range(2)]

    def moved(array, by, other=False):
        return lax.ppermute(
            array,
            "tp",
            [
                (2 * x + core, 2 * ((x + by) % chips) + (1 - core if other else core))
                for x, core in pairs
            ],
        )

    blocks = [block]
    for by in range(1, chips):
        blocks.append(moved(block, by))
    return moved, blocks


def stack_kernel(*refs):
    out_ref = refs[-1]
    for i in range(out_ref.shape[0]):
        out_ref[i] = refs[i][...]


def from_partner(moved, blocks, after):
    stack = pl.pallas_call(
        stack_kernel,
        in_specs=[*whole(len(blocks)), pl.BlockSpec(memory_space=pl.ANY)],
        out_specs=pl.BlockSpec(memory_space=pltpu.VMEM),
        out_shape=jax.ShapeDtypeStruct((len(blocks), *blocks[0].shape), BF16),
        compiler_params=pltpu.CompilerParams(vmem_limit_bytes=VMEM_LIMIT),
        name="stack",
    )
    stacked = stack(*blocks, after)
    return [*blocks, moved(stacked, 0, True)]


def slots_of(me, chips):
    x, core = me // 2, me % 2
    others = [(x + chips - by) % chips for by in range(1, chips)]
    return [
        2 * x + core,
        *[2 * other + core for other in others],
        2 * x + 1 - core,
        *[2 * other + 1 - core for other in others],
    ]


def place(me, block_refs, slots_ref):
    chips = slots_ref.shape[0] // 2
    arrays = [ref[...] for ref in block_refs[:-1]]
    arrays += [block_refs[-1][i] for i in range(chips)]
    for slot, array in zip(slots_of(me, chips), arrays):
        slots_ref[slot] = array


def rows_of(slots_ref, start, count):
    parts = [slots_ref[i, start : start + count, :] for i in range(slots_ref.shape[0])]
    return jnp.concatenate(parts, axis=1)


def next_kernel(q_scale, block_rows, gathered_count, half, *refs):
    me = lax.axis_index("tp")
    block_refs, refs = refs[:gathered_count], refs[gathered_count:]
    x_ref, w_ref, gain_ref, wq_ref, wk_ref, wv_ref, docs_ref, *rest = refs
    q_ref, kv_ref, own_ref, slots_ref, cols_ref = rest
    place(me, block_refs, slots_ref)
    half_rows, col_width = own_ref.shape
    first_row = half * half_rows
    if half == 1:
        kv_ref[half_rows:, :] = doc_rows(docs_ref[:, half_rows:], kv_ref.shape[1])
    for start in range(0, half_rows, block_rows):
        block = slice(start, start + block_rows)
        attended = rows_of(slots_ref, start, block_rows)
        update = jnp.dot(attended, w_ref[...], preferred_element_type=F32)
        rows = x_ref[first_row + start : first_row + start + block_rows, :]
        hidden = (rows.astype(F32) + update).astype(BF16)
        for part in range(cols_ref.shape[0]):
            cols_ref[part, block, :] = hidden[:, part * col_width : (part + 1) * col_width]
        queries, kv = project_heads(
            hidden, gain_ref[1:2, :], wq_ref[...], wk_ref[...], wv_ref[...], q_scale
        )
        q_ref[block, :] = queries
        kv_ref[block, :] = kv
    own_ref[...] = cols_ref[me]


def next_heads(blocks, tokens, w_out, gains, wq, wk, wv, docs, half, q_scale, block_rows=256):
    half_rows, block_width = blocks[0].shape
    depth, width = wq.shape
    inner = w_out.shape[0]
    members = inner // block_width
    col_width = depth // members
    args = [*blocks, tokens, w_out, gains, wq, wk, wv, docs]
    return pl.pallas_call(
        functools.partial(next_kernel, q_scale, block_rows, len(blocks), half),
        in_specs=whole(len(args)),
        out_specs=whole(3),
        out_shape=[
            jax.ShapeDtypeStruct((half_rows, width), BF16),
            jax.ShapeDtypeStruct((half_rows + half * DOC_ROWS, 2 * width), BF16),
            jax.ShapeDtypeStruct((half_rows, col_width), BF16),
        ],
        scratch_shapes=[
            pltpu.VMEM((members, half_rows, block_width), BF16),
            pltpu.VMEM((members, half_rows, col_width), BF16),
        ],
        cost_estimate=cost(
            2 * half_rows * depth * (inner + 3 * width),
            2 * depth * (half_rows + 3 * width + inner),
        ),
        compiler_params=pltpu.CompilerParams(vmem_limit_bytes=VMEM_LIMIT),
        name="next_heads",
    )(*args)


def last_kernel(gathered_count, *refs):
    block_refs, refs = refs[:gathered_count], refs[gathered_count:]
    own_ref, w_ref, out_ref, slots_ref = refs[0], refs[1], refs[-2], refs[-1]
    place(lax.axis_index("tp"), block_refs, slots_ref)
    half_rows = own_ref.shape[0]
    attended = rows_of(slots_ref, 0, half_rows)
    update = jnp.dot(attended, w_ref[...], preferred_element_type=F32)
    out_ref[:half_rows, :] = (own_ref[...].astype(F32) + update).astype(BF16)
    if len(refs) == 5:
        out_ref[half_rows:, :] = refs[2][...]


def last_update(blocks, own, w_out, below=()):
    half_rows, block_width = blocks[0].shape
    inner, col_width = w_out.shape
    args = [*blocks, own, w_out, *below]
    rows = half_rows + sum(array.shape[0] for array in below)
    return pl.pallas_call(
        functools.partial(last_kernel, len(blocks)),
        in_specs=whole(len(args)),
        out_specs=pl.BlockSpec(memory_space=pltpu.VMEM),
        scratch_shapes=[pltpu.VMEM((inner // block_width, half_rows, block_width), BF16)],
        out_shape=jax.ShapeDtypeStruct((rows, col_width), BF16),
        cost_estimate=cost(
            2 * half_rows * inner * col_width, 2 * inner * (half_rows + col_width)
        ),
        compiler_params=pltpu.CompilerParams(vmem_limit_bytes=VMEM_LIMIT),
        name="last",
    )(*args)


def shards(tokens, doc_ids, gains, w_query, w_key, w_value, rel_table, out_first, out_last):
    head_count = rel_table.shape[1]
    width = w_query.shape[2]
    head_width = width // head_count
    q_scale = head_width ** (-0.5) * LOG2E
    members = lax.axis_size("sp")
    onward = [(i, i + 1) for i in range(members - 1)]

    queries, kv_early, kv_late, docs, biases, *weights = heads(
        tokens, gains, w_query, w_key, w_value, doc_ids, rel_table, q_scale
    )
    q_late = q_early = queries
    far = lax.ppermute(kv_late, "sp", onward)
    result = None
    for layer in range(LAYERS):
        late = attention(q_late, kv_early, kv_late, docs, biases, layer, head_width, False)
        moved, late = gather(late)
        ahead = (tokens, out_first) if layer == 0 else (out_last,)
        early = attention(
            q_early, far, kv_early, docs, biases, layer, head_width, True, ahead
        )
        late = from_partner(moved, late, early)
        moved, early = gather(early)
        if layer == 0:
            q_late, kv_late, own_late = next_heads(
                late, tokens, out_first, *weights, docs, 1, q_scale
            )
            far = lax.ppermute(kv_late, "sp", onward)
            early = from_partner(moved, early, kv_late)
            q_early, kv_early, own_early = next_heads(
                early, tokens, out_first, *weights, docs, 0, q_scale
            )
        else:
            below = last_update(late, own_late, out_last)
            early = from_partner(moved, early, below)
            result = last_update(early, own_early, out_last, (below,))
    return result


def solution(mesh):
    placed = (
        P(("grp", "sp"), None),
        P(("grp", "sp")),
        P(),
        P(None, None, "tp"),
        P(None, None, "tp"),
        P(None, None, "tp"),
        P(None, "tp", None),
        P(),
        P(None, "tp"),
    )
    return jax.shard_map(
        shards, mesh=mesh, in_specs=placed, out_specs=P(("grp", "sp"), "tp"), check_vma=False
    )
```

```python
import functools

import jax
import jax.numpy as jnp
from jax import lax
from jax.experimental import pallas as pl
from jax.experimental.pallas import tpu as pltpu
from jax.sharding import PartitionSpec as P


SEG = 64
PREV_SEGS = 8
MAX_REL = 128
LAYERS = 2
REACH = PREV_SEGS * SEG
QUERY_ROWS = 2 * SEG
BAND = REACH + QUERY_ROWS
NEG = -1e30
EPS = 1e-06
LOG2E = 1.4426950408889634
DOC_ROWS = 16
VMEM_LIMIT = 24 * 2**20
FIRST_VMEM_LIMIT = 51 * 2**20


F32 = jnp.float32
BF16 = jnp.bfloat16


def cost(flops, bytes_accessed, transcendentals=0):
    return pl.CostEstimate(
        flops=flops, bytes_accessed=bytes_accessed, transcendentals=transcendentals
    )


def project_heads(rows, gain, wq, wk, wv, q_scale):
    rows32 = rows.astype(F32)
    inv = lax.rsqrt(jnp.mean(rows32 * rows32, axis=-1, keepdims=True) + EPS)
    scaled = rows * gain
    queries = jnp.dot(scaled, wq, preferred_element_type=F32) * (inv * q_scale)
    wkv = jnp.concatenate([wk, wv], axis=1)
    kv = jnp.dot(scaled, wkv, preferred_element_type=F32) * inv
    return queries.astype(BF16), kv.astype(BF16)


def doc_rows(docs, width):
    parts = [docs[:, i : i + width] for i in range(0, docs.shape[1], width)]
    pad = jnp.zeros((DOC_ROWS - len(parts), width), F32)
    return jnp.concatenate(parts + [pad], axis=0).astype(BF16)


def heads_kernel(q_scale, block_rows, *refs):
    x_hbm, gain_hbm, *w_hbm, docs_hbm, table_hbm = refs[:7]
    q_ref, early_ref, late_ref, docs_ref, near_ref, gain_ref, *next_refs = refs[7:16]
    x_ref, *w_refs, ids_ref, table_ref, x_sem, w_sem, next_sem, side_sem = refs[16:]
    row_count = x_ref.shape[0]
    half_rows = row_count // 2
    order = [*range(half_rows, row_count, block_rows), *range(0, half_rows, block_rows)]
    side_copies = [
        pltpu.make_async_copy(source, target, side_sem.at[i])
        for i, (source, target) in enumerate(
            [(docs_hbm, ids_ref), (table_hbm, table_ref), (gain_hbm, gain_ref)]
        )
    ]
    w_copies = [
        pltpu.make_async_copy(w.at[0], w_ref, w_sem.at[i])
        for i, (w, w_ref) in enumerate(zip(w_hbm, w_refs))
    ]
    next_copies = [
        pltpu.make_async_copy(w.at[1], next_ref, next_sem.at[i])
        for i, (w, next_ref) in enumerate(zip(w_hbm, next_refs))
    ]
    x_copies = [
        pltpu.make_async_copy(
            x_hbm.at[pl.ds(row, block_rows)], x_ref.at[pl.ds(row, block_rows)], x_sem.at[i]
        )
        for i, row in enumerate(order)
    ]
    for copy in (*side_copies, x_copies[0], *w_copies, x_copies[1]):
        copy.start()
    for copy in side_copies:
        copy.wait()
    near_bias(table_ref, near_ref)
    docs = (ids_ref[...] + 1).astype(F32)[None, :]
    docs_ref[...] = docs
    width = late_ref.shape[1]
    late_ref[half_rows:, :] = doc_rows(docs[:, half_rows:], width)
    for copy in w_copies:
        copy.wait()
    later = [[copy] for copy in x_copies[2:]] + [next_copies, []]
    for copy, row, starting in zip(x_copies, order, later):
        copy.wait()
        for other in starting:
            other.start()
        queries, kv = project_heads(
            x_ref[pl.ds(row, block_rows), :],
            gain_ref[0:1, :],
            *[w_ref[...] for w_ref in w_refs],
            q_scale,
        )
        q_ref[pl.ds(row, block_rows), :] = queries
        if row < half_rows:
            early_ref[pl.ds(row, block_rows), :] = kv
        else:
            late_ref[pl.ds(row - half_rows, block_rows), :] = kv
    for copy in next_copies:
        copy.wait()


def whole(count):
    return [pl.BlockSpec(memory_space=pltpu.VMEM)] * count


def heads(tokens, gains, wq, wk, wv, doc_ids, rel_table, q_scale, block_rows=256):
    row_count = tokens.shape[0]
    half_rows = row_count // 2
    depth, width = wq.shape[1:]
    items = rel_table.shape[0] * rel_table.shape[1]
    hbm = pl.BlockSpec(memory_space=pltpu.HBM)
    args = [tokens, gains, wq, wk, wv, doc_ids, rel_table]
    args = [pltpu.with_memory_space_constraint(array, pltpu.HBM) for array in args]
    return pl.pallas_call(
        functools.partial(heads_kernel, q_scale, block_rows),
        in_specs=[hbm] * 7,
        out_specs=whole(9),
        out_shape=[
            jax.ShapeDtypeStruct((row_count, width), BF16),
            jax.ShapeDtypeStruct((half_rows, 2 * width), BF16),
            jax.ShapeDtypeStruct((half_rows + DOC_ROWS, 2 * width), BF16),
            jax.ShapeDtypeStruct((1, row_count), F32),
            jax.ShapeDtypeStruct((items, QUERY_ROWS, 2 * MAX_REL), F32),
            jax.ShapeDtypeStruct(gains.shape, BF16),
            *[jax.ShapeDtypeStruct((depth, width), BF16) for _ in range(3)],
        ],
        scratch_shapes=[
            pltpu.VMEM((row_count, depth), BF16),
            *[pltpu.VMEM((depth, width), BF16) for _ in range(3)],
            pltpu.VMEM(doc_ids.shape, doc_ids.dtype),
            pltpu.VMEM(rel_table.shape, F32),
            pltpu.SemaphoreType.DMA((row_count // block_rows,)),
            *[pltpu.SemaphoreType.DMA((3,)) for _ in range(3)],
        ],
        cost_estimate=cost(6 * row_count * depth * width, 2 * depth * (row_count + 3 * width)),
        compiler_params=pltpu.CompilerParams(vmem_limit_bytes=FIRST_VMEM_LIMIT),
        name="heads",
    )(*args)


def near_bias(table_ref, out_ref):
    layers, head_count, table_width = table_ref.shape
    near = 2 * MAX_REL
    width = near + QUERY_ROWS
    index = lax.broadcasted_iota(jnp.int32, (table_width, width), 0)
    place_of = lax.broadcasted_iota(jnp.int32, (table_width, width), 1)
    wanted = jnp.where(place_of < near, near - place_of, near)
    picked = (index == wanted).astype(F32)
    row = lax.broadcasted_iota(jnp.int32, (QUERY_ROWS, near), 0)
    col = lax.broadcasted_iota(jnp.int32, (QUERY_ROWS, near), 1)
    seen = jnp.logical_or(row >= SEG, col < near - SEG)
    for layer in range(layers):
        table = table_ref[layer]
        lines = jnp.dot(
            table, picked, precision=lax.Precision.HIGHEST, preferred_element_type=F32
        )
        lines = (lines - lines[:, near : near + 1]) * LOG2E
        for head in range(head_count):
            spread = jnp.broadcast_to(lines[head : head + 1, :], (QUERY_ROWS, width))
            rolled = pltpu.roll(spread, 0, 1, stride=1, stride_axis=0)
            out_ref[layer * head_count + head] = jnp.where(seen, rolled[:, :near], NEG)


def attention_kernel(head_width, layer, from_far, *refs):
    q_ref, lo_ref, hi_ref, docs_ref, bias_ref, out_ref = (*refs[:5], refs[-1])
    half_rows, width = docs_ref.shape[1] // 2, out_ref.shape[1]
    if out_ref.shape[0] > half_rows:
        out_ref[half_rows:, :] = refs[5][...]
    first_query = 0 if from_far else q_ref.shape[0] - half_rows
    if from_far:
        docs_rows = lo_ref[-DOC_ROWS:, :].astype(F32)
        parts = half_rows // docs_rows.shape[1]
        docs_lo = jnp.concatenate([docs_rows[i : i + 1] for i in range(parts)], axis=1)
        docs_hi = docs_ref[:, :half_rows]
    else:
        docs_lo = docs_ref[:, :half_rows]
        docs_hi = docs_ref[:, half_rows:]
    head_count = width // head_width
    lane = lax.broadcasted_iota(jnp.int32, (QUERY_ROWS, width), 1) // head_width
    square = (QUERY_ROWS, QUERY_ROWS)
    diagonal = lax.broadcasted_iota(jnp.int32, square, 0) == lax.broadcasted_iota(
        jnp.int32, square, 1
    )
    seen = jnp.logical_or(
        lax.broadcasted_iota(jnp.int32, square, 0) < SEG,
        lax.broadcasted_iota(jnp.int32, square, 1) >= SEG,
    )
    ones = jnp.ones((BAND, width), BF16)
    chunks = BAND // QUERY_ROWS
    plain = chunks - bias_ref.shape[2] // QUERY_ROWS
    first_head = layer * head_count
    for block in range(half_rows // QUERY_ROWS):
        start = block * QUERY_ROWS
        stop = start + QUERY_ROWS
        kv = jnp.concatenate([lo_ref[start:half_rows, :], hi_ref[:stop, :]], axis=0)
        docs_keys = jnp.concatenate([docs_lo[:, start:], docs_hi[:, :stop]], axis=1)
        docs_queries = jnp.sum(
            jnp.where(diagonal, docs_hi[:, start:stop], 0.0), axis=1, keepdims=True
        )
        same = []
        for c in range(chunks):
            keys = docs_keys[:, c * QUERY_ROWS : (c + 1) * QUERY_ROWS]
            if c == 0:
                keys = jnp.where(seen, keys, -1.0)
            same.append(keys == docs_queries)
        queries = q_ref[first_query + start : first_query + stop, :]
        zero = jnp.zeros_like(queries)
        stacked = jnp.concatenate(
            [jnp.where(lane == head, queries, zero) for head in range(head_count)], axis=0
        )
        scores = lax.dot_general(
            stacked, kv[:, :width], (((1,), (1,)), ((), ())), preferred_element_type=F32
        )
        weights = []
        for head in range(head_count):
            parts = []
            for c in range(chunks):
                part = scores[
                    head * QUERY_ROWS : (head + 1) * QUERY_ROWS,
                    c * QUERY_ROWS : (c + 1) * QUERY_ROWS,
                ]
                if c >= plain:
                    near = (c - plain) * QUERY_ROWS
                    part = part + bias_ref[first_head + head, :, near : near + QUERY_ROWS]
                parts.append(jnp.where(same[c], part, NEG))
            top = jnp.max(functools.reduce(jnp.maximum, parts), axis=1, keepdims=True)
            weights.append(
                jnp.concatenate([jnp.exp2(part - top).astype(BF16) for part in parts], axis=1)
            )
        weights = jnp.concatenate(weights, axis=0)
        summed = jnp.dot(
            weights,
            jnp.concatenate([kv[:, width:], ones], axis=1),
            preferred_element_type=F32,
        )
        result = summed[:, :width] / summed[:, width:]
        mine = result[:QUERY_ROWS]
        for head in range(1, head_count):
            mine = jnp.where(lane == head, result[head * QUERY_ROWS : (head + 1) * QUERY_ROWS], mine)
        out_ref[start:stop, :] = mine.astype(BF16)


def attention(queries, lo, hi, docs, biases, layer, head_width, from_far, ahead=(), below=()):
    half_rows = docs.shape[1] // 2
    width = queries.shape[1]
    return pl.pallas_call(
        functools.partial(attention_kernel, head_width, layer, from_far),
        in_specs=whole(5 + len(below) + len(ahead)),
        out_specs=pl.BlockSpec(memory_space=pltpu.VMEM),
        out_shape=jax.ShapeDtypeStruct((half_rows * (1 + len(below)), width), BF16),
        cost_estimate=cost(400 * half_rows * BAND * width, 8 * half_rows * width, half_rows * BAND * 2),
        compiler_params=pltpu.CompilerParams(vmem_limit_bytes=VMEM_LIMIT),
        name="attend",
    )(queries, lo, hi, docs, biases, *below, *ahead)


def gather(block, order=(1, 2, 3)):
    chips = lax.axis_size("tp") // 2
    pairs = [(x, core) for x in range(chips) for core in range(2)]

    def moved(array, by, other=False):
        return lax.ppermute(
            array,
            "tp",
            [
                (2 * x + core, 2 * ((x + by) % chips) + (1 - core if other else core))
                for x, core in pairs
            ],
        )

    blocks = [block]
    for by in order:
        blocks.append(moved(block, by))
    return moved, blocks


def stack_kernel(*refs):
    out_ref = refs[-1]
    for i in range(out_ref.shape[0]):
        out_ref[i] = refs[i][...]


def from_partner(moved, blocks, after):
    stack = pl.pallas_call(
        stack_kernel,
        in_specs=[*whole(len(blocks)), pl.BlockSpec(memory_space=pl.ANY)],
        out_specs=pl.BlockSpec(memory_space=pltpu.VMEM),
        out_shape=jax.ShapeDtypeStruct((len(blocks), *blocks[0].shape), BF16),
        compiler_params=pltpu.CompilerParams(vmem_limit_bytes=VMEM_LIMIT),
        name="stack",
    )
    stacked = stack(*blocks, after)
    return [*blocks, moved(stacked, 0, True)]


def slots_of(me, chips):
    x, core = me // 2, me % 2
    others = [(x + chips - by) % chips for by in range(1, chips)]
    return [
        2 * x + core,
        *[2 * other + core for other in others],
        2 * x + 1 - core,
        *[2 * other + 1 - core for other in others],
    ]


def place(me, block_refs, slots_ref):
    chips = slots_ref.shape[0] // 2
    arrays = [ref[...] for ref in block_refs[:-1]]
    arrays += [block_refs[-1][i] for i in range(chips)]
    for slot, array in zip(slots_of(me, chips), arrays):
        slots_ref[slot] = array


def rows_of(slots_ref, start, count):
    parts = [slots_ref[i, start : start + count, :] for i in range(slots_ref.shape[0])]
    return jnp.concatenate(parts, axis=1)


def next_kernel(q_scale, block_rows, gathered_count, half, *refs):
    me = lax.axis_index("tp")
    block_refs, refs = refs[:gathered_count], refs[gathered_count:]
    x_ref, w_ref, gain_ref, wq_ref, wk_ref, wv_ref, docs_ref, *rest = refs
    q_ref, kv_ref, own_ref, slots_ref, cols_ref = rest
    place(me, block_refs, slots_ref)
    half_rows, col_width = own_ref.shape
    first_row = half * half_rows
    if half == 1:
        kv_ref[half_rows:, :] = doc_rows(docs_ref[:, half_rows:], kv_ref.shape[1])
    for start in range(0, half_rows, block_rows):
        block = slice(start, start + block_rows)
        attended = rows_of(slots_ref, start, block_rows)
        update = jnp.dot(attended, w_ref[...], preferred_element_type=F32)
        rows = x_ref[first_row + start : first_row + start + block_rows, :]
        hidden = (rows.astype(F32) + update).astype(BF16)
        for part in range(cols_ref.shape[0]):
            cols_ref[part, block, :] = hidden[:, part * col_width : (part + 1) * col_width]
        queries, kv = project_heads(
            hidden, gain_ref[1:2, :], wq_ref[...], wk_ref[...], wv_ref[...], q_scale
        )
        q_ref[block, :] = queries
        kv_ref[block, :] = kv
    own_ref[...] = cols_ref[me]


def next_heads(blocks, tokens, w_out, gains, wq, wk, wv, docs, half, q_scale, block_rows=256):
    half_rows, block_width = blocks[0].shape
    depth, width = wq.shape
    inner = w_out.shape[0]
    members = inner // block_width
    col_width = depth // members
    args = [*blocks, tokens, w_out, gains, wq, wk, wv, docs]
    return pl.pallas_call(
        functools.partial(next_kernel, q_scale, block_rows, len(blocks), half),
        in_specs=whole(len(args)),
        out_specs=whole(3),
        out_shape=[
            jax.ShapeDtypeStruct((half_rows, width), BF16),
            jax.ShapeDtypeStruct((half_rows + half * DOC_ROWS, 2 * width), BF16),
            jax.ShapeDtypeStruct((half_rows, col_width), BF16),
        ],
        scratch_shapes=[
            pltpu.VMEM((members, half_rows, block_width), BF16),
            pltpu.VMEM((members, half_rows, col_width), BF16),
        ],
        cost_estimate=cost(
            2 * half_rows * depth * (inner + 3 * width),
            2 * depth * (half_rows + 3 * width + inner),
        ),
        compiler_params=pltpu.CompilerParams(vmem_limit_bytes=VMEM_LIMIT),
        name="next_heads",
    )(*args)


def last_kernel(near_count, *refs):
    *block_refs, early_ref, late_ref, w_ref, out_ref, slots_ref = refs
    members = slots_ref.shape[0]
    slots = slots_of(lax.axis_index("tp"), members // 2)
    near_refs, near_partners, far_ref, far_partner = (
        block_refs[:near_count],
        block_refs[near_count],
        block_refs[-2],
        block_refs[-1],
    )
    sources = [0, 1, members // 2 - 1]
    for i, source in enumerate(sources):
        slots_ref[slots[source]] = near_refs[i][...]
        slots_ref[slots[members // 2 + source]] = near_partners[i]
    slots_ref[slots[2]] = far_ref[...]
    slots_ref[slots[members // 2 + 2]] = far_partner[...]
    half_rows = early_ref.shape[0]
    for start, own_ref in ((0, early_ref), (half_rows, late_ref)):
        attended = rows_of(slots_ref, start, half_rows)
        update = jnp.dot(attended, w_ref[...], preferred_element_type=F32)
        rows = own_ref[...].astype(F32) + update
        out_ref[start : start + half_rows, :] = rows.astype(BF16)


def last_update(attended, early, late, w_out):
    moved, blocks = gather(attended, (1, 3, 2))
    near, far = blocks[:3], blocks[3]
    near = from_partner(moved, near, near[0])
    args = [*near, far, moved(far, 0, True), early, late, w_out]
    rows, block_width = attended.shape
    inner, col_width = w_out.shape
    return pl.pallas_call(
        functools.partial(last_kernel, len(near) - 1),
        in_specs=whole(len(args)),
        out_specs=pl.BlockSpec(memory_space=pltpu.VMEM),
        scratch_shapes=[pltpu.VMEM((inner // block_width, rows, block_width), BF16)],
        out_shape=jax.ShapeDtypeStruct((rows, col_width), BF16),
        cost_estimate=cost(2 * rows * inner * col_width, 2 * inner * (rows + col_width)),
        compiler_params=pltpu.CompilerParams(vmem_limit_bytes=VMEM_LIMIT),
        name="last",
    )(*args)


def shards(tokens, doc_ids, gains, w_query, w_key, w_value, rel_table, out_first, out_last):
    head_count = rel_table.shape[1]
    width = w_query.shape[2]
    head_width = width // head_count
    q_scale = head_width ** (-0.5) * LOG2E
    members = lax.axis_size("sp")
    onward = [(i, i + 1) for i in range(members - 1)]

    queries, kv_early, kv_late, docs, biases, *weights = heads(
        tokens, gains, w_query, w_key, w_value, doc_ids, rel_table, q_scale
    )
    q_late = q_early = queries
    far = lax.ppermute(kv_late, "sp", onward)
    result = None
    for layer in range(LAYERS):
        late = attention(q_late, kv_early, kv_late, docs, biases, layer, head_width, False)
        if layer == LAYERS - 1:
            attended = attention(
                q_early, far, kv_early, docs, biases, layer, head_width, True,
                (out_last,), (late,),
            )
            result = last_update(attended, own_early, own_late, out_last)
            break
        moved, late = gather(late)
        early = attention(
            q_early, far, kv_early, docs, biases, layer, head_width, True, (tokens, out_first)
        )
        late = from_partner(moved, late, early)
        moved, early = gather(early)
        q_late, kv_late, own_late = next_heads(late, tokens, out_first, *weights, docs, 1, q_scale)
        far = lax.ppermute(kv_late, "sp", onward)
        early = from_partner(moved, early, kv_late)
        q_early, kv_early, own_early = next_heads(
            early, tokens, out_first, *weights, docs, 0, q_scale
        )
    return result


def solution(mesh):
    placed = (
        P(("grp", "sp"), None),
        P(("grp", "sp")),
        P(),
        P(None, None, "tp"),
        P(None, None, "tp"),
        P(None, None, "tp"),
        P(None, "tp", None),
        P(),
        P(None, "tp"),
    )
    return jax.shard_map(
        shards, mesh=mesh, in_specs=placed, out_specs=P(("grp", "sp"), "tp"), check_vma=False
    )
```
